256 devices in a mesh: sp: 64 (over z, x, core), tp: 4 (over y).
Axes of the slice: x: 4, y: 4, z: 8, core: 2. Of those that a mesh axis runs over, the one named last changes fastest.
Arguments:
- layer_input: bfloat16 [8192, 2048], P('sp', 'tp'), may hold values from -6 to 6
- cotangent: bfloat16 [8192, 2048], P('sp', 'tp'), may hold values from -16 to 16
- routes: int32 [8192, 2], P('sp'), may hold values from 0 to 63, all different within a row; in each aligned block of 128 rows (0 to 127, 128 to 255, ...) at most 6 rows name the same one
- route_weight: float32 [8192, 2], P('sp'), may hold values from 0.1 to 0.6
- gate_weight: bfloat16 [64, 2048, 1024], P('sp', None, 'tp'), may hold values from -0.125 to 0.125
- up_weight: bfloat16 [64, 2048, 1024], P('sp', None, 'tp'), may hold values from -0.125 to 0.125
- down_weight: bfloat16 [64, 1024, 2048], P('sp', 'tp'), may hold values from -0.1875 to 0.1875
- heads_value: bfloat16 [8192, 2048], P('sp', 'tp'), may hold values from -6 to 6
- output_gate: bfloat16 [8192, 2048], P('sp', 'tp'), may hold values from -8 to 8
- mixer_saved: bfloat16 [8192, 2048], P('sp', 'tp'), may hold values from -6 to 6
- proj_weight: bfloat16 [2048, 2048], P(None, 'tp'), may hold values from -0.125 to 0.125
- state_write: bfloat16 [8192, 512], P('sp', 'tp'), may hold values from -0.5 to 0.5
- state_read: bfloat16 [8192, 512], P('sp', 'tp'), may hold values from -0.5 to 0.5
- decay_rate: float32 [8192, 32], P('sp', 'tp'), may hold values from 0 to 1.1, as said below
Outputs:
- gate_grad: bfloat16 [64, 2048, 1024], P('sp', None, 'tp')
- up_grad: bfloat16 [64, 2048, 1024], P('sp', None, 'tp')
- down_grad: bfloat16 [64, 1024, 2048], P('sp', 'tp')
- proj_grad: float32 [2048, 2048], P('sp', 'tp')
- value_grad: bfloat16 [8192, 2048], P('sp', 'tp')
- write_gradient: bfloat16 [8192, 512], P('sp', 'tp')
- read_gradient: bfloat16 [8192, 512], P('sp', 'tp')
- outgate_grad: bfloat16 [8192, 2048], P('sp', 'tp')
The draws below stay inside these ranges and needn't reach their ends.
Inputs may be any that keep to these rules, and one draw needn't show every extreme that they name: `routes`: each row names 2 different experts; within the rows of one aligned block of 128 tokens no expert is named by more than 6 rows, a bound that some block reaches. `decay_rate`: positive log-decays.
All inputs are finite; a program needn't handle non-finite values.
Results may differ from the reference program's by a relative error of at most 0.017.
Values may be sent and summed in bfloat16 or wider, within the bound.
No kernel may reach another device: no remote copies, remote signals or barrier semaphores. Data moves between devices by JAX's collectives and lax.ppermute only.
A program may use at most 128 MiB of HBM per device.

```python
import math
import jax
import jax.numpy as jnp
import numpy as np
from jax import lax

D = 2048
BLENDER_CHANNEL = 32
HEAD_DIM = 64
GROUPS = 4
STATE = 128
EXP_HIDDEN = 1024
TOPK = 2
TOK_DEV = 128
SERIES_ENTRIES = 8192
EXPERTS = 64
CAP = 6
SSD_W = 2048
N_SP = 64
N_TP = 4


def draw_decay_rate(key, part):
    address_rows = jax.random.split(jax.random.fold_in(key, 11), 5)
    share = 0.5
    fast_heads = jax.random.uniform(address_rows[0], (BLENDER_CHANNEL,), jnp.float32) < share
    random_noise = jax.random.uniform(address_rows[1], (SERIES_ENTRIES, BLENDER_CHANNEL), jnp.float32, 0.5, 1.5)
    block_multiplier = jax.random.uniform(address_rows[2], (SERIES_ENTRIES // TOK_DEV, 1, 1), jnp.float32, 0.5, 1.5)
    block_multiplier = jnp.broadcast_to(block_multiplier, (SERIES_ENTRIES // TOK_DEV, TOK_DEV, 1)).reshape(SERIES_ENTRIES, 1)
    baseline_rate = jnp.where(fast_heads, 0.03, 0.5 / SERIES_ENTRIES)[None, :]
    interval_starts = jax.random.randint(address_rows[3], (2, BLENDER_CHANNEL), 0, SERIES_ENTRIES)
    interval_spans = jax.random.uniform(address_rows[4], (2, BLENDER_CHANNEL), jnp.float32, 0.22, 0.5)
    entry_indices = jnp.arange(SERIES_ENTRIES, dtype=jnp.int32)[:, None]
    pulse_clusters = jnp.where(entry_indices == interval_starts[0][None, :], interval_spans[0][None, :], 0.0)
    pulse_clusters = pulse_clusters + jnp.where(entry_indices == interval_starts[1][None, :], interval_spans[1][None, :], 0.0)
    pulse_clusters = jnp.where(fast_heads[None, :], 0.0, pulse_clusters)
    return (baseline_rate * random_noise * block_multiplier + pulse_clusters).astype(jnp.float32)


def raised(result, rng, source, target, shards_of, factor):
    def block_of(dim):
        return (jnp.arange(result.shape[dim]) // (result.shape[dim] // shards_of)).reshape((-1,) + (1,) * (result.ndim - 1 - dim))

    first = jax.random.permutation(rng, shards_of)[block_of(target)]
    second = (block_of(target) + shards_of // 2) % shards_of
    return jnp.where((block_of(source) == first) | (block_of(source) == second), factor * result, result)


def steps_of(rng, shape, cuts, least, high):
    def one(dim, blocks):
        heights = jax.random.uniform(jax.random.fold_in(jax.random.fold_in(rng, 6), dim), (blocks,), jnp.float32, least / len(cuts), high / len(cuts))
        return jnp.repeat(jnp.exp(heights), shape[dim] // blocks).reshape((-1,) + (1,) * (len(shape) - dim - 1))

    gain = one(*cuts[0])
    for cut in cuts[1:]:
        gain = gain * one(*cut)
    return gain


def deal_out(rng, own, number, rows, count, top, reach, skew):
    order = jax.random.permutation(rng, count)
    heavy_load, usual = shares(count, rows * top, reach, skew, True), shares(count, rows * top, reach, skew, False)
    places = jnp.arange(count)

    def named(tallies, offset_by):
        used = int((tallies > 0).sum())
        fixed = max(1, used // 4)
        moved = fixed + (places - fixed + offset_by * (used - fixed)) % max(1, count - fixed)
        return jnp.zeros((count,), jnp.int32).at[order[jnp.where(places < fixed, places, moved)]].set(jnp.asarray(tallies, jnp.int32))

    tallies = jnp.where(number % 4 == 0, named(heavy_load, number // 4), named(usual, number - number // 4 - 1))
    mixed = jax.random.permutation(jax.random.fold_in(own, 3), count)
    donor, taker = mixed[0:count // 2 * 2:2], mixed[1:count // 2 * 2:2]
    room = jnp.minimum(tallies[donor] - 1, reach - tallies[taker]) // 2
    room = jnp.where((donor == order[0]) | (taker == order[0]) | (tallies[taker] == 0), 0, jnp.maximum(room, 0))
    moved = jax.random.randint(jax.random.fold_in(own, 4), (count // 2,), 0, 1 << 20) % (room + 1)
    tallies = tallies.at[donor].add(-moved).at[taker].add(moved)
    items = jnp.searchsorted(jnp.cumsum(tallies), jnp.arange(rows * top), side="right").astype(jnp.int32)
    grid = items.reshape(top, rows).T
    grid = grid[jax.random.permutation(jax.random.fold_in(own, 1), rows)]
    offset_by = jax.random.randint(jax.random.fold_in(own, 2), (rows, 1), 0, top)
    return jnp.take_along_axis(grid, (jnp.arange(top)[None, :] + offset_by) % top, axis=1)


def shares(number_of, total, most, lean, full):
    weights = [(1 << 20) // math.isqrt(standing ** lean) + 1 for standing in range(1, number_of + 1)]
    largest = most if full else min(most, max(-(-total // number_of), total * weights[0] // sum(weights)))
    least = 1 if total - largest >= number_of - 1 else 0
    counts, surplus = [largest] + [least] * (number_of - 1), total - largest - least * (number_of - 1)
    while surplus > 0:
        free = [i for i in range(1, number_of) if counts[i] < largest] or [i for i in range(1, number_of) if counts[i] < most]
        pool, left = sum([weights[i] for i in free]), surplus
        for i in free:
            addition = min(most - counts[i], max(1, left * weights[i] // pool), surplus)
            counts[i] = counts[i] + addition
            surplus = surplus - addition
    return np.array(counts)


def gaussian(key, shape, deviation, limit, cuts=(), held_as=jnp.bfloat16):
    drawn = deviation * jax.random.normal(key, shape, jnp.float32)
    if cuts:
        drawn = drawn * steps_of(key, shape, cuts, -0.22, 0.18)
    return jnp.clip(drawn, -limit, limit).astype(held_as)


def heavy_noise(own_key, extent, deviation, reach, shards, heavy, held_as=jnp.bfloat16):
    array = deviation * jax.random.normal(own_key, extent, jnp.float32)
    if shards:
        array = array * steps_of(own_key, extent, shards, -0.22, 0.18)
    return jnp.clip(raised(array, jax.random.fold_in(own_key, 3), *heavy), -reach, reach).astype(held_as)


def setup_inputs(seed: int = 0) -> dict:
    seeds = jax.random.split(jax.random.key(seed), 15)
    layer_input = gaussian(seeds[0], (SERIES_ENTRIES, D), 1.0, 6.0, ((0, 64), (1, 4)))
    cotangent = heavy_noise(seeds[1], (SERIES_ENTRIES, D), 1.0, 16.0, ((0, 64), (1, 4)), (0, 1, 64, 4.0))
    routes_keys = jax.random.split(jax.random.fold_in(seeds[2], 1), SERIES_ENTRIES // TOK_DEV)
    routes_turns = jax.random.permutation(jax.random.fold_in(seeds[2], 3), SERIES_ENTRIES // TOK_DEV)
    routes = jax.vmap(lambda own, number: deal_out(jax.random.fold_in(seeds[2], 2), own, number, TOK_DEV, EXPERTS, TOPK, CAP, 1))(routes_keys, routes_turns).reshape((SERIES_ENTRIES, TOPK))
    route_weight = jnp.clip(0.1 + 0.5 * jax.random.uniform(seeds[3], (SERIES_ENTRIES, TOPK), jnp.float32) ** steps_of(seeds[3], (SERIES_ENTRIES, TOPK), ((0, 64),), -0.2, 0.2), 0.1, 0.6)
    gate_weight = gaussian(seeds[4], (EXPERTS, D, EXP_HIDDEN), D ** -0.5, 0.125, ((0, 64), (2, 4)))
    up_weight = gaussian(seeds[5], (EXPERTS, D, EXP_HIDDEN), D ** -0.5, 0.125, ((0, 64), (2, 4)))
    down_weight = gaussian(seeds[6], (EXPERTS, EXP_HIDDEN, D), EXP_HIDDEN ** -0.5, 0.1875, ((0, 64), (1, 4)))
    heads_value = gaussian(seeds[7], (SERIES_ENTRIES, SSD_W), 1.0, 6.0, ((0, 64), (1, 4)))
    output_gate = gaussian(seeds[8], (SERIES_ENTRIES, SSD_W), 1.5, 8.0, ((0, 64), (1, 4)))
    mixer_saved = gaussian(seeds[9], (SERIES_ENTRIES, SSD_W), 1.0, 6.0, ((0, 64), (1, 4)))
    proj_weight = gaussian(seeds[10], (D, SSD_W), SSD_W ** -0.5, 0.125, ((1, 4),))
    state_write = gaussian(seeds[11], (SERIES_ENTRIES, GROUPS * STATE), 0.08, 0.5, ((0, 64), (1, 4)))
    state_read = gaussian(seeds[12], (SERIES_ENTRIES, GROUPS * STATE), 0.08, 0.5, ((0, 64), (1, 4)))
    decay_rate = draw_decay_rate(jax.random.fold_in(seeds[14], 71), 0)
    return dict(layer_input=layer_input, cotangent=cotangent, routes=routes, route_weight=route_weight, gate_weight=gate_weight, up_weight=up_weight, down_weight=down_weight, heads_value=heads_value, output_gate=output_gate, mixer_saved=mixer_saved, proj_weight=proj_weight, state_write=state_write, state_read=state_read, decay_rate=decay_rate)


maximal_value = lax.Precision.HIGHEST


def silu_parts(value):
    sigma = jax.nn.sigmoid(value)
    return value * sigma, sigma * (1.0 + value * (1.0 - sigma))


def slot_index(flat_routes):
    onehot = (flat_routes[:, None] == jnp.arange(EXPERTS, dtype=jnp.int32)[None, :]).astype(jnp.int32)
    before = jnp.cumsum(onehot, axis=0, dtype=jnp.int32) - onehot
    ranks = jnp.sum(before * onehot, axis=1, dtype=jnp.int32)
    return (flat_routes * CAP + ranks).astype(jnp.int32)


def block_sums(block):
    value_vectors, step_deltas, write_vectors, read_vectors, rates = block
    repeat = BLENDER_CHANNEL // GROUPS
    cumul = jnp.cumsum(rates, axis=0)
    total = cumul[-1]
    to_end = jnp.exp(cumul - total)
    to_start = jnp.exp(-cumul)
    write_heads = jnp.repeat(write_vectors, repeat, axis=1)
    read_heads = jnp.repeat(read_vectors, repeat, axis=1)
    write_end = jnp.einsum('shn,shp->hnp', write_heads * to_end[:, :, None], value_vectors, precision=maximal_value)
    read_end = jnp.einsum('shn,shp->hnp', read_heads * to_end[:, :, None], step_deltas, precision=maximal_value)
    write_start = jnp.einsum('shn,shp->hnp', write_heads * to_start[:, :, None], value_vectors, precision=maximal_value)
    read_start = jnp.einsum('shn,shp->hnp', read_heads * to_start[:, :, None], step_deltas, precision=maximal_value)
    return total, write_end, read_end, write_start, read_start


def block_grads(item):
    value_vectors, step_deltas, write_vectors, read_vectors, rates, write_low, read_low, write_high, read_high = item
    repeat = BLENDER_CHANNEL // GROUPS
    length = value_vectors.shape[0]
    cumul = jnp.cumsum(rates, axis=0)
    to_end = jnp.exp(cumul - cumul[-1])
    to_start = jnp.exp(-cumul)
    write_heads = jnp.repeat(write_vectors, repeat, axis=1)
    read_heads = jnp.repeat(read_vectors, repeat, axis=1)
    mixing_kernel = jnp.exp(-jnp.abs(cumul.T[:, :, None] - cumul.T[:, None, :]))
    common_part = jnp.repeat(jnp.einsum('tgn,sgn->gts', read_vectors, write_vectors, precision=maximal_value), repeat, axis=0)
    match_scores = jnp.einsum('thp,shp->hts', step_deltas, value_vectors, precision=maximal_value)
    weighted_values = mixing_kernel * match_scores
    value_g = jnp.einsum('hts,thp->shp', mixing_kernel * common_part, step_deltas, precision=maximal_value)
    write_g = jnp.einsum('hts,thn->shn', weighted_values, read_heads, precision=maximal_value)
    read_g = jnp.einsum('hts,shn->thn', weighted_values, write_heads, precision=maximal_value)
    value_g = value_g + jnp.einsum('hnp,thn->thp', read_low, write_heads, precision=maximal_value) * to_start[:, :, None]
    value_g = value_g + jnp.einsum('hnp,thn->thp', read_high, write_heads, precision=maximal_value) * to_end[:, :, None]
    write_g = write_g + jnp.einsum('hnp,thp->thn', read_low, value_vectors * to_start[:, :, None], precision=maximal_value)
    write_g = write_g + jnp.einsum('hnp,thp->thn', read_high, value_vectors * to_end[:, :, None], precision=maximal_value)
    read_g = read_g + jnp.einsum('hnp,thp->thn', write_low, step_deltas * to_start[:, :, None], precision=maximal_value)
    read_g = read_g + jnp.einsum('hnp,thp->thn', write_high, step_deltas * to_end[:, :, None], precision=maximal_value)
    write_g = write_g.reshape(length, GROUPS, repeat, STATE).sum(axis=2)
    read_g = read_g.reshape(length, GROUPS, repeat, STATE).sum(axis=2)
    return value_g, write_g, read_g


def reference(layer_input, cotangent, routes, route_weight, gate_weight, up_weight, down_weight,
              heads_value, output_gate, mixer_saved, proj_weight, state_write, state_read, decay_rate):
    flat = routes.reshape(N_SP, TOK_DEV * TOPK)
    slots = jax.vmap(slot_index)(flat)
    owners = jnp.arange(TOK_DEV * TOPK, dtype=jnp.int32) // TOPK
    offsets = (jnp.arange(N_SP, dtype=jnp.int32) * TOK_DEV)[:, None]

    def slot_tokens(slot_row, offset_row):
        return jnp.full((EXPERTS * CAP,), SERIES_ENTRIES, jnp.int32).at[slot_row].set(owners + offset_row)

    def slot_weights(slot_row, weight_row):
        return jnp.zeros((EXPERTS * CAP,), jnp.float32).at[slot_row].set(weight_row)

    token_table = jax.vmap(slot_tokens)(slots, offsets)
    weight_table = jax.vmap(slot_weights)(slots, route_weight.reshape(N_SP, TOK_DEV * TOPK))
    token_table = token_table.reshape(N_SP, EXPERTS, CAP).transpose(1, 0, 2).reshape(EXPERTS, N_SP * CAP)
    weight_table = weight_table.reshape(N_SP, EXPERTS, CAP).transpose(1, 0, 2).reshape(EXPERTS, N_SP * CAP)
    inputs_pad = jnp.concatenate([layer_input, jnp.zeros((1, D), layer_input.dtype)], axis=0)
    cotangent_pad = jnp.concatenate([cotangent, jnp.zeros((1, D), cotangent.dtype)], axis=0)
    width = EXP_HIDDEN // N_TP

    def expert_step(item):
        rows, weights, gate_one, up_one, down_one = item
        inputs = inputs_pad[rows]
        sent = (cotangent_pad[rows].astype(jnp.float32) * weights[:, None]).astype(jnp.bfloat16)
        pre_gate = jnp.dot(inputs, gate_one, preferred_element_type=jnp.float32)
        pre_up = jnp.dot(inputs, up_one, preferred_element_type=jnp.float32)
        active, slope = silu_parts(pre_gate)
        hidden = (active * pre_up).astype(jnp.bfloat16)
        hidden_grad = jnp.dot(sent, down_one.T, preferred_element_type=jnp.float32)
        gate_delta = (hidden_grad * pre_up * slope).astype(jnp.bfloat16)
        up_delta = (hidden_grad * active).astype(jnp.bfloat16)
        down_g = jnp.dot(hidden.T, sent, preferred_element_type=jnp.float32).astype(jnp.bfloat16)
        gate_g = jnp.dot(inputs.T, gate_delta, preferred_element_type=jnp.float32).astype(jnp.bfloat16)
        up_g = jnp.dot(inputs.T, up_delta, preferred_element_type=jnp.float32).astype(jnp.bfloat16)
        parts = jnp.einsum('rjk,djk->jrd', gate_delta.reshape(-1, N_TP, width).astype(jnp.float32),
                           gate_one.reshape(D, N_TP, width).astype(jnp.float32))
        parts = parts + jnp.einsum('rjk,djk->jrd', up_delta.reshape(-1, N_TP, width).astype(jnp.float32),
                                   up_one.reshape(D, N_TP, width).astype(jnp.float32))
        rounded = lax.optimization_barrier(parts.astype(jnp.bfloat16)).astype(jnp.float32)
        returned = jnp.sum(rounded, axis=0).astype(jnp.bfloat16)
        return gate_g, up_g, down_g, returned

    gate_grad, up_grad, down_grad, returned = lax.map(
        expert_step, (token_table, weight_table, gate_weight, up_weight, down_weight))
    expert_of = slots // CAP
    rank_of = slots % CAP
    sources = jnp.arange(N_SP, dtype=jnp.int32)[:, None]
    position = (expert_of * (N_SP * CAP) + sources * CAP + rank_of).astype(jnp.int32).reshape(-1)
    moe_grad = returned.reshape(-1, D)[position].astype(jnp.float32).reshape(SERIES_ENTRIES, TOPK, D).sum(axis=1)
    layer_grad = (cotangent.astype(jnp.float32) + moe_grad).astype(jnp.bfloat16)

    out_delta = jnp.dot(layer_grad, proj_weight, preferred_element_type=jnp.float32).astype(jnp.bfloat16)
    active_gate, slope_gate = silu_parts(output_gate.astype(jnp.float32))
    saved = mixer_saved.astype(jnp.float32)
    gated = (saved * active_gate).astype(jnp.bfloat16)
    proj_grad = jnp.dot(layer_grad.T, gated, preferred_element_type=jnp.float32)
    outgate_grad = (out_delta.astype(jnp.float32) * saved * slope_gate).astype(jnp.bfloat16)
    mixer_delta = out_delta.astype(jnp.float32) * active_gate

    blk = math.gcd(TOK_DEV, 256)
    count = SERIES_ENTRIES // blk
    value_vectors = heads_value.astype(jnp.float32).reshape(count, blk, BLENDER_CHANNEL, HEAD_DIM)
    step_deltas = mixer_delta.reshape(count, blk, BLENDER_CHANNEL, HEAD_DIM)
    write_vectors = state_write.astype(jnp.float32).reshape(count, blk, GROUPS, STATE)
    read_vectors = state_read.astype(jnp.float32).reshape(count, blk, GROUPS, STATE)
    rates = decay_rate.astype(jnp.float32).reshape(count, blk, BLENDER_CHANNEL)
    totals, write_end, read_end, write_start, read_start = lax.map(block_sums, (value_vectors, step_deltas, write_vectors, read_vectors, rates))
    zero_state = jnp.zeros((BLENDER_CHANNEL, STATE, HEAD_DIM), jnp.float32)

    def carry_on(state, item):
        total, write_part, read_part = item
        fade = jnp.exp(-total)[:, None, None]
        return (fade * state[0] + write_part, fade * state[1] + read_part), state

    _, (write_low, read_low) = lax.scan(carry_on, (zero_state, zero_state), (totals, write_end, read_end))
    _, (write_high, read_high) = lax.scan(carry_on, (zero_state, zero_state), (totals, write_start, read_start), reverse=True)
    value_g, write_g, read_g = lax.map(block_grads, (value_vectors, step_deltas, write_vectors, read_vectors, rates,
                                                     write_low, read_low, write_high, read_high))
    return (gate_grad, up_grad, down_grad, proj_grad,
            value_g.reshape(SERIES_ENTRIES, SSD_W).astype(jnp.bfloat16),
            write_g.reshape(SERIES_ENTRIES, GROUPS * STATE).astype(jnp.bfloat16),
            read_g.reshape(SERIES_ENTRIES, GROUPS * STATE).astype(jnp.bfloat16),
            outgate_grad)
```

```python
import jax
import jax.numpy as jnp
from jax import lax
from jax.experimental import pallas as pl
from jax.sharding import Mesh
from jax.sharding import PartitionSpec as P


HEAD_DIM = 64
STATE = 128
SP = ("sp_0", "sp_1", "sp_2")
CHIPS = ("sp_0", "sp_1")
CORE = "sp_2"
TP = "tp"

f32 = jnp.float32
bf16 = jnp.bfloat16


def dot(a, b, ca=1, cb=0):
    return lax.dot_general(a, b, (((ca,), (cb,)), ((), ())), preferred_element_type=f32)


def swap(x):
    return lax.ppermute(x, CORE, [(0, 1), (1, 0)])


def ring(x, shift):
    n = lax.axis_size(TP)
    return lax.ppermute(x, TP, [(i, (i + shift) % n) for i in range(n)])


def exchange(x):
    return lax.all_to_all(x, CHIPS, split_axis=0, concat_axis=0, tiled=True)


def silu_parts(value):
    sigma = jax.nn.sigmoid(value)
    return (value * sigma, sigma * (1.0 + value * (1.0 - sigma)))


def scan_kernel(msg_ref, fade_ref, out_ref, work_ref):
    chunks = msg_ref.shape[0]
    work_ref[...] = msg_ref[...].astype(f32)
    low = jnp.zeros((8, 128), f32)
    high = jnp.zeros((8, 128), f32)
    for i in range(chunks):
        k = chunks - 1 - i
        own_low = work_ref[i, 0:8, :]
        own_high = work_ref[k, 8:16, :]
        work_ref[i, 0:8, :] = low
        work_ref[k, 8:16, :] = high
        low = low * fade_ref[i : i + 1, :] + own_low
        high = high * fade_ref[k : k + 1, :] + own_high
    out_ref[...] = work_ref[...].astype(bf16)


def scan_chunks(msg, fade):
    from jax.experimental.pallas import tpu as pltpu

    return pl.pallas_call(
        scan_kernel,
        out_shape=jax.ShapeDtypeStruct(msg.shape, bf16),
        scratch_shapes=[pltpu.VMEM(msg.shape, f32)],
    )(msg, fade)


def to_message(low, high):
    def cut(a):
        n, w = a.shape
        return a.astype(bf16).reshape(n // 8, 8, w // 128, 128).transpose(2, 0, 1, 3)

    both = jnp.stack([cut(low), cut(high)], axis=2)
    return both.reshape(-1, 16, 128)


def from_message(msg, width):
    parts = msg.reshape(width // 128, STATE // 8, 2, 8, 128)
    return tuple(
        parts[:, :, d].reshape(width // 128, STATE, 128).transpose(1, 0, 2).reshape(STATE, width)
        for d in range(2)
    )


def on_device(
    layer_input,
    cotangent,
    routes,
    route_weight,
    gate_weight,
    up_weight,
    down_weight,
    heads_value,
    output_gate,
    mixer_saved,
    proj_weight,
    state_write,
    state_read,
    decay_rate,
):
    core = lax.axis_index(CORE)
    tp = lax.axis_index(TP)
    first = core == 0
    tokens, width = layer_input.shape
    chips = lax.axis_size(CHIPS)
    experts = 2 * chips
    cap = max(2, 3 * tokens * routes.shape[1] // (2 * experts))
    rows = 2 * cap
    n_tp = lax.axis_size(TP)
    heads = decay_rate.shape[1]
    half_heads = heads // 2
    half = heads_value.shape[1] // 2

    def ordered(mine, other, axis=0):
        return jnp.concatenate(
            [jnp.where(first, mine, other), jnp.where(first, other, mine)], axis=axis
        )

    def halves(a):
        left, right = a[:, : a.shape[1] // 2], a[:, a.shape[1] // 2 :]
        return jnp.where(first, left, right), jnp.where(first, right, left)

    small = jnp.concatenate([routes.astype(f32), route_weight, decay_rate], axis=1)
    small_other = swap(small)
    input_other = swap(layer_input)
    cotangent_other = swap(cotangent)
    active_gate, slope_gate = silu_parts(output_gate.astype(f32))
    saved = mixer_saved.astype(f32)
    gated = (saved * active_gate).astype(bf16)
    value_mine, value_send = halves(heads_value)
    gated_mine, gated_send = halves(gated)
    side = jnp.concatenate([value_send, gated_send, state_write, state_read], axis=1)
    side_other = swap(side)

    both = jnp.concatenate([small, small_other], axis=0)
    turned = both[:, :4].T
    routes_row = turned[0:2].astype(jnp.int32)
    weight_row = turned[2:4]
    count = 2 * tokens
    token_row = lax.broadcasted_iota(jnp.int32, (1, count), 1)
    source_row = token_row // tokens
    expert_col = lax.broadcasted_iota(jnp.int32, (experts, count), 0)
    named = [expert_col == routes_row[k : k + 1] for k in range(2)]
    named_any = (named[0] | named[1]).astype(bf16)
    earlier = lax.broadcasted_iota(jnp.int32, (count, count), 0)
    later = lax.broadcasted_iota(jnp.int32, (count, count), 1)
    before_mask = ((earlier < later) & (earlier // tokens == later // tokens)).astype(bf16)
    before = dot(named_any, before_mask)
    place = []
    for k in range(2):
        rank = jnp.sum(jnp.where(named[k], before, 0.0), axis=0, keepdims=True).astype(jnp.int32)
        expert = routes_row[k : k + 1]
        here = expert % 2 == core
        place.append(
            (jnp.where(here, expert // 2, -1), source_row * cap + rank)
        )
    out_col = lax.broadcasted_iota(jnp.int32, (chips * 2 * rows, 2 * count), 0)
    pick = None
    scale = None
    for k in range(2):
        chip, inner = place[k]
        spot = jnp.where(chip < 0, -1, chip * (2 * rows) + inner)
        spots = jnp.concatenate([spot, jnp.where(spot < 0, -1, spot + rows)], axis=1)
        factor = jnp.concatenate([jnp.ones_like(weight_row[k : k + 1]), weight_row[k : k + 1]], axis=1)
        hit = out_col == spots
        part = jnp.where(hit, factor, 0.0)
        pick = hit if pick is None else pick | hit
        scale = part if scale is None else scale + part
    scale = jnp.sum(scale, axis=1, keepdims=True)
    stacked = jnp.concatenate([layer_input, input_other, cotangent, cotangent_other], axis=0)
    sent = (dot(pick.astype(bf16), stacked) * scale).astype(bf16)
    received = exchange(sent.reshape(chips, 2 * rows, width))

    back_col = lax.broadcasted_iota(jnp.int32, (chips * rows, count), 0)
    back = None
    for k in range(2):
        chip, inner = place[k]
        hit = back_col == jnp.where(chip < 0, -1, chip * rows + inner)
        back = hit if back is None else back | hit
    back = back.astype(bf16)

    value = ordered(value_mine, side_other[:, :half])
    gated_all = jnp.concatenate([gated_mine, side_other[:, half : 2 * half]], axis=0)
    write = ordered(state_write, side_other[:, 2 * half : 2 * half + STATE])
    read = ordered(state_read, side_other[:, 2 * half + STATE :])
    rates_mine = small[:, 4:]
    rates_other = small_other[:, 4:]
    rates = ordered(halves(rates_mine)[0], halves(rates_other)[0])
    cumul = jnp.cumsum(rates, axis=0)
    spread = (
        lax.broadcasted_iota(jnp.int32, (half_heads, half), 1) // HEAD_DIM
        == lax.broadcasted_iota(jnp.int32, (half_heads, half), 0)
    ).astype(f32)
    cumul_wide = jnp.dot(cumul, spread, precision=lax.Precision.HIGHEST)
    total_wide = cumul_wide[-1:]
    fade_end = jnp.exp(cumul_wide - total_wide)
    fade_start = jnp.exp(-cumul_wide)
    value_f = value.astype(f32)
    value_end = (value_f * fade_end).astype(bf16)
    value_start = (value_f * fade_start).astype(bf16)
    write_states = to_message(dot(write, value_end, 0, 0), dot(write, value_start, 0, 0))
    total_high = lax.reduce_precision(total_wide, 8, 7)
    total_rows = jnp.concatenate(
        [total_high, total_wide - total_high, jnp.zeros((6, half), f32)], axis=0
    ).astype(bf16)
    total_rows = jnp.broadcast_to(
        total_rows.reshape(8, half // 128, 1, 128).transpose(1, 2, 0, 3),
        (half // 128, STATE // 8, 8, 128),
    ).reshape(-1, 8, 128)
    write_sent = jnp.concatenate([write_states, total_rows], axis=1)
    write_sent, received = lax.optimization_barrier((write_sent, received))
    write_got = exchange(write_sent)
    totals = write_got[:, 16].astype(f32) + write_got[:, 17].astype(f32)
    fade_chunk = jnp.exp(-totals)
    write_scanned = scan_chunks(write_got[:, :16], fade_chunk)

    quarter = width
    step = tp * quarter

    def rolled(a):
        return lax.dynamic_slice_in_dim(jnp.concatenate([a, a], axis=0), step, a.shape[0], 0)

    def unrolled(a):
        start = (n_tp - tp) % n_tp * quarter
        return lax.dynamic_slice_in_dim(jnp.concatenate([a, a], axis=0), start, a.shape[0], 0)

    gate_up = rolled(jnp.concatenate([gate_weight[0], up_weight[0]], axis=1))
    down = [
        lax.dynamic_slice_in_dim(down_weight[0], (tp + i) % n_tp * quarter, quarter, 1)
        for i in range(n_tp)
    ]
    proj = rolled(proj_weight)
    hid = gate_weight.shape[2]
    slots = chips * rows
    hs = slots // 2

    def gather(a):
        low = ring(a, 1)
        up = ring(a, -1)
        far_low = ring(low[:hs], 1)
        far_up = ring(up[hs:], -1)
        return a, up, jnp.concatenate([far_low, far_up], axis=0), low

    input_parts = gather(received[:, :rows].reshape(slots, width))
    cotangent_parts = gather(received[:, rows:].reshape(slots, width))
    expert_input = jnp.concatenate(input_parts, axis=1)
    pre = dot(expert_input, gate_up)
    pre_gate, pre_up = pre[:, :hid], pre[:, hid:]
    active, slope = silu_parts(pre_gate)
    hidden = (active * pre_up).astype(bf16)
    hidden_grad = sum(dot(cotangent_parts[i], down[i], 1, 1) for i in range(n_tp))
    deltas = jnp.concatenate(
        [(hidden_grad * pre_up * slope).astype(bf16), (hidden_grad * active).astype(bf16)], axis=1
    )
    partial = dot(deltas, gate_up, 1, 1).astype(bf16)
    partial, write_scanned = lax.optimization_barrier((partial, write_scanned))
    write_back = exchange(write_scanned)
    own, right, far, left = (partial[:, i * quarter : (i + 1) * quarter] for i in range(n_tp))
    from_left = ring(far[:hs], 1).astype(f32)
    from_right = ring(far[hs:], -1).astype(f32)
    to_right = jnp.concatenate(
        [(right[:hs].astype(f32) + from_left).astype(bf16), right[hs:]], axis=0
    )
    to_left = jnp.concatenate(
        [left[:hs], (left[hs:].astype(f32) + from_right).astype(bf16)], axis=0
    )
    returned = (
        own.astype(f32) + ring(to_right, 1).astype(f32) + ring(to_left, -1).astype(f32)
    ).astype(bf16)
    arrived = exchange(returned.reshape(chips, rows, width)).reshape(slots, width)

    both_grad = unrolled(dot(expert_input, deltas, 0, 0).astype(bf16))
    gate_grad = both_grad[:, :hid][None]
    up_grad = both_grad[:, hid:][None]
    down_parts = jnp.stack([dot(hidden, cotangent_parts[i], 0, 0).astype(bf16) for i in range(n_tp)])
    down_grad = jnp.concatenate(
        [
            lax.dynamic_index_in_dim(down_parts, (k - tp) % n_tp, 0, keepdims=False)
            for k in range(n_tp)
        ],
        axis=1,
    )[None]

    summed = dot(back, arrived, 0, 0)
    summed_other = swap(summed[tokens:].astype(bf16)).astype(f32)
    layer_grad = (cotangent.astype(f32) + summed[:tokens] + summed_other).astype(bf16)
    full_grad = jnp.concatenate(
        [layer_grad, ring(layer_grad, -1), ring(layer_grad, 2), ring(layer_grad, 1)], axis=1
    )
    out_delta = dot(full_grad, proj).astype(bf16).astype(f32)
    outgate_grad = (out_delta * saved * slope_gate).astype(bf16)
    mixer_delta = (out_delta * active_gate).astype(bf16)
    delta_mine, delta_send = halves(mixer_delta)
    delta = ordered(delta_mine, swap(delta_send))
    delta_f = delta.astype(f32)
    delta_end = (delta_f * fade_end).astype(bf16)
    delta_start = (delta_f * fade_start).astype(bf16)
    read_sent = to_message(dot(read, delta_end, 0, 0), dot(read, delta_start, 0, 0))
    read_back = exchange(scan_chunks(exchange(read_sent), fade_chunk))

    grad_all = jnp.concatenate([full_grad, swap(full_grad)], axis=0)
    proj_part = unrolled(dot(grad_all, gated_all, 0, 0).astype(bf16))
    per_chip = proj_part.shape[0] // chips
    proj_got = exchange(proj_part.reshape(chips, per_chip, half))
    proj_sum = jnp.sum(proj_got.astype(f32), axis=0)
    top, bottom = proj_sum[: per_chip // 2], proj_sum[per_chip // 2 :]
    proj_mine = jnp.where(first, top, bottom)
    proj_grad = ordered(proj_mine, swap(jnp.where(first, bottom, top)), axis=1)

    cumul_row = cumul.T
    common = dot(read, write, 1, 1)
    score = None
    value_parts = []
    for h in range(half_heads):
        mix = jnp.exp(-jnp.abs(cumul[:, h : h + 1] - cumul_row[h : h + 1]))
        lanes = slice(h * HEAD_DIM, (h + 1) * HEAD_DIM)
        match = dot(delta[:, lanes], value[:, lanes], 1, 1) * mix
        score = match if score is None else score + match
        value_parts.append(dot((mix * common).astype(bf16), delta[:, lanes], 0, 0))
    score = score.astype(bf16)
    write_low, write_high = from_message(write_back, half)
    read_low, read_high = from_message(read_back, half)
    value_grad = (
        jnp.concatenate(value_parts, axis=1)
        + dot(write, read_low) * fade_start
        + dot(write, read_high) * fade_end
    )
    write_grad = (
        dot(score, read, 0, 0) + dot(value_start, read_low, 1, 1) + dot(value_end, read_high, 1, 1)
    )
    read_grad = (
        dot(score, write) + dot(delta_start, write_low, 1, 1) + dot(delta_end, write_high, 1, 1)
    )
    outs = jnp.concatenate([value_grad, write_grad, read_grad], axis=1)
    outs_mine = jnp.where(first, outs[:tokens], outs[tokens:])
    outs_got = swap(jnp.where(first, outs[tokens:], outs[:tokens]).astype(bf16))
    value_out = ordered(outs_mine[:, :half].astype(bf16), outs_got[:, :half], axis=1)
    sums = (outs_mine[:, half:] + outs_got[:, half:].astype(f32)).astype(bf16)
    return (
        gate_grad,
        up_grad,
        down_grad,
        proj_grad,
        value_out,
        sums[:, :STATE],
        sums[:, STATE:],
        outgate_grad,
    )


def solution(mesh):
    split = Mesh(mesh.devices.reshape(8, 4, 2, mesh.shape["tp"]), SP + (TP,))
    placed = (
        P(SP, TP),
        P(SP, TP),
        P(SP, None),
        P(SP, None),
        P(SP, None, TP),
        P(SP, None, TP),
        P(SP, TP, None),
        P(SP, TP),
        P(SP, TP),
        P(SP, TP),
        P(None, TP),
        P(SP, TP),
        P(SP, TP),
        P(SP, TP),
    )
    return jax.shard_map(
        on_device,
        mesh=split,
        in_specs=placed,
        out_specs=(
            P(SP, None, TP),
            P(SP, None, TP),
            P(SP, TP, None),
            P(SP, TP),
            P(SP, TP),
            P(SP, TP),
            P(SP, TP),
            P(SP, TP),
        ),
        check_vma=False,
    )
```

```python
import jax
import jax.numpy as jnp
from jax import lax
from jax.experimental import pallas as pl
from jax.sharding import Mesh
from jax.sharding import PartitionSpec as P


HEAD_DIM = 64
STATE = 128
SP = ("sp_0", "sp_1", "sp_2")
CHIPS = ("sp_0", "sp_1")
CORE = "sp_2"
TP = "tp"

f32 = jnp.float32
bf16 = jnp.bfloat16


def dot(a, b, ca=1, cb=0):
    return lax.dot_general(a, b, (((ca,), (cb,)), ((), ())), preferred_element_type=f32)


def swap(x):
    return lax.ppermute(x, CORE, [(0, 1), (1, 0)])


def ring(x, shift, axis=TP):
    n = lax.axis_size(axis)
    return lax.ppermute(x, axis, [(i, (i + shift) % n) for i in range(n)])


def ring_reduce(parts, axis):
    own, right, far, left = parts
    h = own.shape[0] // 2
    from_left = ring(far[:h], 1, axis).astype(f32)
    from_right = ring(far[h:], -1, axis).astype(f32)
    to_right = jnp.concatenate([(right[:h].astype(f32) + from_left).astype(bf16), right[h:]], axis=0)
    to_left = jnp.concatenate([left[:h], (left[h:].astype(f32) + from_right).astype(bf16)], axis=0)
    return (
        own.astype(f32)
        + ring(to_right, 1, axis).astype(f32)
        + ring(to_left, -1, axis).astype(f32)
    )


def exchange(x):
    return lax.all_to_all(x, CHIPS, split_axis=0, concat_axis=0, tiled=True)


def silu_parts(value):
    sigma = jax.nn.sigmoid(value)
    return (value * sigma, sigma * (1.0 + value * (1.0 - sigma)))


def scan_kernel(msg_ref, fade_ref, out_ref, work_ref):
    chunks, height, _ = msg_ref.shape
    work_ref[...] = msg_ref[...].astype(f32)
    states = [jnp.zeros((8, 128), f32)] * (height // 8)
    for i in range(chunks):
        for s in range(height // 8):
            k = i if s % 2 == 0 else chunks - 1 - i
            rows = slice(s * 8, s * 8 + 8)
            own = work_ref[k, rows, :]
            work_ref[k, rows, :] = states[s]
            states[s] = states[s] * fade_ref[k : k + 1, :] + own
    out_ref[...] = work_ref[...].astype(bf16)


def scan_chunks(msg, fade):
    from jax.experimental.pallas import tpu as pltpu

    return pl.pallas_call(
        scan_kernel,
        out_shape=jax.ShapeDtypeStruct(msg.shape, bf16),
        scratch_shapes=[pltpu.VMEM(msg.shape, f32)],
    )(msg, fade)


def to_message(low, high):
    def cut(a):
        n, w = a.shape
        return a.astype(bf16).reshape(n // 8, 8, w // 128, 128).transpose(2, 0, 1, 3)

    both = jnp.stack([cut(low), cut(high)], axis=2)
    return both.reshape(-1, 16, 128)


def from_message(msg, width):
    parts = msg.reshape(width // 128, STATE // 8, 2, 8, 128)
    return tuple(
        parts[:, :, d].reshape(width // 128, STATE, 128).transpose(1, 0, 2).reshape(STATE, width)
        for d in range(2)
    )


def on_device(
    layer_input,
    cotangent,
    routes,
    route_weight,
    gate_weight,
    up_weight,
    down_weight,
    heads_value,
    output_gate,
    mixer_saved,
    proj_weight,
    state_write,
    state_read,
    decay_rate,
):
    core = lax.axis_index(CORE)
    tp = lax.axis_index(TP)
    first = core == 0
    tokens, width = layer_input.shape
    chips = lax.axis_size(CHIPS)
    experts = 2 * chips
    cap = max(2, 3 * tokens * routes.shape[1] // (2 * experts))
    rows = 2 * cap
    n_tp = lax.axis_size(TP)
    heads = decay_rate.shape[1]
    half_heads = heads // 2
    half = heads_value.shape[1] // 2

    def ordered(mine, other, axis=0):
        return jnp.concatenate(
            [jnp.where(first, mine, other), jnp.where(first, other, mine)], axis=axis
        )

    def halves(a):
        left, right = a[:, : a.shape[1] // 2], a[:, a.shape[1] // 2 :]
        return jnp.where(first, left, right), jnp.where(first, right, left)

    routes_other = swap(routes)
    weight_other = swap(route_weight)
    input_other = swap(layer_input)
    cotangent_other = swap(cotangent)

    routes_row = jnp.concatenate([routes.T, routes_other.T], axis=1)
    weight_row = jnp.concatenate([route_weight.T, weight_other.T], axis=1)
    count = 2 * tokens
    token_row = lax.broadcasted_iota(jnp.int32, (1, count), 1)
    source_row = (token_row >= tokens).astype(jnp.int32)
    expert_col = lax.broadcasted_iota(jnp.int32, (experts, count), 0)
    named = [expert_col == routes_row[k : k + 1] for k in range(2)]
    named_any = (named[0] | named[1]).astype(bf16)
    earlier = lax.broadcasted_iota(jnp.int32, (count, count), 0)
    later = lax.broadcasted_iota(jnp.int32, (count, count), 1)
    before_mask = ((earlier < later) & ((earlier < tokens) == (later < tokens))).astype(bf16)
    before = dot(named_any, before_mask)
    place = []
    for k in range(2):
        rank = jnp.sum(jnp.where(named[k], before, 0.0), axis=0, keepdims=True).astype(jnp.int32)
        expert = routes_row[k : k + 1]
        here = (expert & 1) == core
        place.append(
            (jnp.where(here, expert >> 1, -1), source_row * cap + rank)
        )
    out_col = lax.broadcasted_iota(jnp.int32, (chips * 2 * rows, 2 * count), 0)
    pick = None
    scale = None
    for k in range(2):
        chip, inner = place[k]
        spot = jnp.where(chip < 0, -1, chip * (2 * rows) + inner)
        spots = jnp.concatenate([spot, jnp.where(spot < 0, -1, spot + rows)], axis=1)
        factor = jnp.concatenate([jnp.ones_like(weight_row[k : k + 1]), weight_row[k : k + 1]], axis=1)
        hit = out_col == spots
        part = jnp.where(hit, factor, 0.0)
        pick = hit if pick is None else pick | hit
        scale = part if scale is None else scale + part
    scale = jnp.sum(scale, axis=1, keepdims=True)
    stacked = jnp.concatenate([layer_input, input_other, cotangent, cotangent_other], axis=0)
    sent = (dot(pick.astype(bf16), stacked) * scale).astype(bf16)
    later_inputs = (gate_weight, up_weight, down_weight, heads_value, output_gate, mixer_saved)
    later_inputs += (proj_weight, state_write, state_read, decay_rate)
    sent, later_inputs = lax.optimization_barrier((sent, later_inputs))
    gate_weight, up_weight, down_weight, heads_value, output_gate, mixer_saved = later_inputs[:6]
    proj_weight, state_write, state_read, decay_rate = later_inputs[6:]
    received = exchange(sent.reshape(chips, 2 * rows, width))

    back_col = lax.broadcasted_iota(jnp.int32, (chips * rows, count), 0)
    back = None
    for k in range(2):
        chip, inner = place[k]
        hit = back_col == jnp.where(chip < 0, -1, chip * rows + inner)
        back = hit if back is None else back | hit
    back = back.astype(bf16)

    active_gate, slope_gate = silu_parts(output_gate.astype(f32))
    saved = mixer_saved.astype(f32)
    gated = (saved * active_gate).astype(bf16)
    value_mine, value_send = halves(heads_value)
    gated_mine, gated_send = halves(gated)
    side = jnp.concatenate([value_send, gated_send, state_write, state_read], axis=1)
    side_other = swap(side)
    rates_mine, rates_send = halves(decay_rate)
    value = ordered(value_mine, side_other[:, :half])
    gated_all = jnp.concatenate([gated_mine, side_other[:, half : 2 * half]], axis=0)
    write = ordered(state_write, side_other[:, 2 * half : 2 * half + STATE])
    read = ordered(state_read, side_other[:, 2 * half + STATE :])
    rates = ordered(rates_mine, swap(rates_send))
    cumul = jnp.cumsum(rates, axis=0)
    spread = (
        lax.broadcasted_iota(jnp.int32, (half_heads, half), 1) // HEAD_DIM
        == lax.broadcasted_iota(jnp.int32, (half_heads, half), 0)
    ).astype(f32)
    cumul_wide = jnp.dot(cumul, spread, precision=lax.Precision.HIGHEST)
    total_wide = cumul_wide[-1:]
    fade_end = jnp.exp(cumul_wide - total_wide)
    fade_start = jnp.exp(-cumul_wide)
    value_f = value.astype(f32)
    value_end = (value_f * fade_end).astype(bf16)
    value_start = (value_f * fade_start).astype(bf16)
    write_states = to_message(dot(write, value_end, 0, 0), dot(write, value_start, 0, 0))
    total_high = lax.reduce_precision(total_wide, 8, 7)
    total_rows = jnp.concatenate(
        [total_high, total_wide - total_high, jnp.zeros((6, half), f32)], axis=0
    ).astype(bf16)
    total_rows = jnp.broadcast_to(
        total_rows.reshape(8, half // 128, 1, 128).transpose(1, 2, 0, 3),
        (half // 128, STATE // 8, 8, 128),
    ).reshape(-1, 8, 128)
    quarter = width
    step = tp * quarter

    def rolled(a):
        return lax.dynamic_slice_in_dim(jnp.concatenate([a, a], axis=0), step, a.shape[0], 0)

    def unrolled(a):
        start = ((n_tp - tp) & (n_tp - 1)) * quarter
        return lax.dynamic_slice_in_dim(jnp.concatenate([a, a], axis=0), start, a.shape[0], 0)

    gate_up = rolled(jnp.concatenate([gate_weight[0], up_weight[0]], axis=1))
    down = [
        lax.dynamic_slice_in_dim(down_weight[0], ((tp + i) & (n_tp - 1)) * quarter, quarter, 1)
        for i in range(n_tp)
    ]
    proj = [
        lax.dynamic_slice_in_dim(proj_weight, ((tp + i) & (n_tp - 1)) * quarter, quarter, 0)
        for i in range(n_tp)
    ]
    hid = gate_weight.shape[2]
    slots = chips * rows
    hs = slots // 2

    def gather(a):
        low = ring(a, 1)
        up = ring(a, -1)
        far_low = ring(low[:hs], 1)
        far_up = ring(up[hs:], -1)
        return a, up, jnp.concatenate([far_low, far_up], axis=0), low

    input_parts = gather(received[:, :rows].reshape(slots, width))
    cotangent_parts = gather(received[:, rows:].reshape(slots, width))
    expert_input = jnp.concatenate(input_parts, axis=1)
    pre = dot(expert_input, gate_up)
    pre_gate, pre_up = pre[:, :hid], pre[:, hid:]
    active, slope = silu_parts(pre_gate)
    hidden = (active * pre_up).astype(bf16)
    hidden_grad = sum(dot(cotangent_parts[i], down[i], 1, 1) for i in range(n_tp))
    deltas = jnp.concatenate(
        [(hidden_grad * pre_up * slope).astype(bf16), (hidden_grad * active).astype(bf16)], axis=1
    )
    partial = dot(deltas, gate_up, 1, 1).astype(bf16)
    ready = (write, read, value, gated_all, cumul, fade_end, fade_start, value_end, value_start)
    ready += (write_states, total_rows)
    partial, ready = lax.optimization_barrier((partial, ready))
    write, read, value, gated_all, cumul, fade_end, fade_start, value_end, value_start = ready[:9]
    write_states, total_rows = ready[9:]
    returned = ring_reduce(
        [partial[:, i * quarter : (i + 1) * quarter] for i in range(n_tp)], TP
    ).astype(bf16)
    arrived = exchange(returned.reshape(chips, rows, width)).reshape(slots, width)

    both_grad = unrolled(dot(expert_input, deltas, 0, 0).astype(bf16))
    gate_grad = both_grad[:, :hid][None]
    up_grad = both_grad[:, hid:][None]
    down_parts = jnp.stack([dot(hidden, cotangent_parts[i], 0, 0).astype(bf16) for i in range(n_tp)])
    down_grad = jnp.concatenate(
        [
            lax.dynamic_index_in_dim(down_parts, (k + n_tp - tp) & (n_tp - 1), 0, keepdims=False)
            for k in range(n_tp)
        ],
        axis=1,
    )[None]

    summed = dot(back, arrived, 0, 0)
    summed_other = swap(summed[tokens:].astype(bf16)).astype(f32)
    layer_grad = (cotangent.astype(f32) + summed[:tokens] + summed_other).astype(bf16)
    grads = [layer_grad, ring(layer_grad, -1), ring(layer_grad, 2), ring(layer_grad, 1)]
    out_delta = sum(dot(grads[i], proj[i]) for i in (0, 1, 3, 2)).astype(bf16).astype(f32)
    outgate_grad = (out_delta * saved * slope_gate).astype(bf16)
    mixer_delta = (out_delta * active_gate).astype(bf16)
    delta_mine, delta_send = halves(mixer_delta)
    delta = ordered(delta_mine, swap(delta_send))
    delta_f = delta.astype(f32)
    delta_end = (delta_f * fade_end).astype(bf16)
    delta_start = (delta_f * fade_start).astype(bf16)
    read_states = to_message(dot(read, delta_end, 0, 0), dot(read, delta_start, 0, 0))
    states_got = exchange(jnp.concatenate([read_states, write_states, total_rows], axis=1))
    totals = states_got[:, 32].astype(f32) + states_got[:, 33].astype(f32)
    states_back = exchange(scan_chunks(states_got[:, :32], jnp.exp(-totals)))
    read_back, write_back = states_back[:, :16], states_back[:, 16:]

    grad_mine = jnp.concatenate(grads, axis=1)
    grad_all = jnp.concatenate([grad_mine, swap(grad_mine)], axis=0)
    proj_part = unrolled(dot(grad_all, gated_all, 0, 0).astype(bf16))
    deep, wide = lax.axis_size(SP[0]), lax.axis_size(SP[1])
    block = proj_part.shape[0] // chips
    proj_part = proj_part.reshape(deep, wide, block, half)
    across = lax.axis_index(SP[1])
    proj_part = lax.dynamic_slice_in_dim(
        jnp.concatenate([proj_part, proj_part], axis=1), across, wide, 1
    )
    proj_sum = ring_reduce([proj_part[:, i] for i in range(wide)], SP[1])
    depth = lax.axis_index(SP[0])
    gap = deep // 2
    while gap:
        upper = (depth & gap) != 0
        below, above = proj_sum[:gap], proj_sum[gap:]
        away = jnp.where(upper, below, above).astype(bf16)
        got = lax.ppermute(away, SP[0], [(i, i ^ gap) for i in range(deep)])
        proj_sum = jnp.where(upper, above, below) + got.astype(f32)
        gap //= 2
    proj_sum = proj_sum[0]
    top, bottom = proj_sum[: block // 2], proj_sum[block // 2 :]
    proj_mine = jnp.where(first, top, bottom)
    proj_grad = ordered(proj_mine, swap(jnp.where(first, bottom, top)), axis=1)

    cumul_row = cumul.T
    common = dot(read, write, 1, 1)
    score = None
    value_parts = []
    for h in range(half_heads):
        mix = jnp.exp(-jnp.abs(cumul[:, h : h + 1] - cumul_row[h : h + 1]))
        lanes = slice(h * HEAD_DIM, (h + 1) * HEAD_DIM)
        match = dot(delta[:, lanes], value[:, lanes], 1, 1) * mix
        score = match if score is None else score + match
        value_parts.append(dot((mix * common).astype(bf16), delta[:, lanes], 0, 0))
    score = score.astype(bf16)
    write_low, write_high = from_message(write_back, half)
    read_low, read_high = from_message(read_back, half)
    value_grad = (
        jnp.concatenate(value_parts, axis=1)
        + dot(write, read_low) * fade_start
        + dot(write, read_high) * fade_end
    )
    write_grad = (
        dot(score, read, 0, 0) + dot(value_start, read_low, 1, 1) + dot(value_end, read_high, 1, 1)
    )
    read_grad = (
        dot(score, write) + dot(delta_start, write_low, 1, 1) + dot(delta_end, write_high, 1, 1)
    )
    outs = jnp.concatenate([value_grad, write_grad, read_grad], axis=1)
    outs_mine = jnp.where(first, outs[:tokens], outs[tokens:])
    outs_got = swap(jnp.where(first, outs[tokens:], outs[:tokens]).astype(bf16))
    value_out = ordered(outs_mine[:, :half].astype(bf16), outs_got[:, :half], axis=1)
    sums = (outs_mine[:, half:] + outs_got[:, half:].astype(f32)).astype(bf16)
    return (
        gate_grad,
        up_grad,
        down_grad,
        proj_grad,
        value_out,
        sums[:, :STATE],
        sums[:, STATE:],
        outgate_grad,
    )


def solution(mesh):
    split = Mesh(mesh.devices.reshape(8, 4, 2, mesh.shape["tp"]), SP + (TP,))
    placed = (
        P(SP, TP),
        P(SP, TP),
        P(SP, None),
        P(SP, None),
        P(SP, None, TP),
        P(SP, None, TP),
        P(SP, TP, None),
        P(SP, TP),
        P(SP, TP),
        P(SP, TP),
        P(None, TP),
        P(SP, TP),
        P(SP, TP),
        P(SP, TP),
    )
    return jax.shard_map(
        on_device,
        mesh=split,
        in_specs=placed,
        out_specs=(
            P(SP, None, TP),
            P(SP, None, TP),
            P(SP, TP, None),
            P(SP, TP),
            P(SP, TP),
            P(SP, TP),
            P(SP, TP),
            P(SP, TP),
        ),
        check_vma=False,
    )
```

```python
import jax
import jax.numpy as jnp
from jax import lax
from jax.experimental import pallas as pl
from jax.experimental.pallas import tpu as pltpu
from jax.sharding import Mesh
from jax.sharding import PartitionSpec as P


HEAD_DIM = 64
STATE = 128
SP = ("sp_0", "sp_1", "sp_2")
CHIPS = ("sp_0", "sp_1")
CORE = "sp_2"
TP = "tp"

f32 = jnp.float32
bf16 = jnp.bfloat16


def dot(a, b, ca=1, cb=0):
    return lax.dot_general(a, b, (((ca,), (cb,)), ((), ())), preferred_element_type=f32)


def swap(x):
    return lax.ppermute(x, CORE, [(0, 1), (1, 0)])


def ring(x, shift, axis=TP):
    n = lax.axis_size(axis)
    return lax.ppermute(x, axis, [(i, (i + shift) % n) for i in range(n)])


def ring_reduce(parts, axis):
    own, right, far, left = parts
    opposite = ring(far, 2, axis)
    low = ring(right, 1, axis)
    up = ring(left, -1, axis)
    return own.astype(f32) + low.astype(f32) + up.astype(f32) + opposite.astype(f32)


def exchange(x):
    return lax.all_to_all(x, CHIPS, split_axis=0, concat_axis=0, tiled=True)


def silu_parts(value):
    sigma = jax.nn.sigmoid(value)
    return (value * sigma, sigma * (1.0 + value * (1.0 - sigma)))


def scan_kernel(msg_ref, out_ref, work_ref):
    chunks, height, _ = out_ref.shape
    work_ref[...] = msg_ref[...].astype(f32)
    fades = [
        jnp.exp(-(work_ref[k, height : height + 1, :] + work_ref[k, height + 1 : height + 2, :]))
        for k in range(chunks)
    ]
    states = [jnp.zeros((8, 128), f32)] * (height // 8)
    for i in range(chunks):
        for s in range(height // 8):
            k = i if s % 2 == 0 else chunks - 1 - i
            rows = slice(s * 8, s * 8 + 8)
            own = work_ref[k, rows, :]
            work_ref[k, rows, :] = states[s]
            states[s] = states[s] * fades[k] + own
    out_ref[...] = work_ref[:, :height, :].astype(bf16)


def scan_chunks(msg):
    chunks, height, lanes = msg.shape
    return pl.pallas_call(
        scan_kernel,
        out_shape=jax.ShapeDtypeStruct((chunks, height - 8, lanes), bf16),
        scratch_shapes=[pltpu.VMEM(msg.shape, f32)],
    )(msg)


def tail_kernel(
    core_ref,
    back_ref,
    write_ref,
    value_start_ref,
    value_end_ref,
    delta_start_ref,
    delta_end_ref,
    fade_start_ref,
    fade_end_ref,
    base_ref,
    mine_ref,
    send_ref,
    work_ref,
):
    blocks = value_start_ref.shape[1] // 128
    steps = back_ref.shape[0] // blocks
    half = blocks * 128
    write = write_ref[...]
    write_sum = base_ref[:, half : half + STATE]
    read_sum = base_ref[:, half + STATE :]
    for q in range(blocks):
        states = back_ref[q * steps : (q + 1) * steps].astype(f32)
        read_low, read_high, write_low, write_high = (
            states[:, 8 * i : 8 * i + 8, :].reshape(STATE, 128).astype(bf16) for i in range(4)
        )
        lanes = slice(q * 128, (q + 1) * 128)
        work_ref[:, lanes] = (
            base_ref[:, lanes]
            + dot(write, read_low) * fade_start_ref[:, lanes]
            + dot(write, read_high) * fade_end_ref[:, lanes]
        )
        write_sum = write_sum + dot(value_start_ref[:, lanes], read_low, 1, 1)
        write_sum = write_sum + dot(value_end_ref[:, lanes], read_high, 1, 1)
        read_sum = read_sum + dot(delta_start_ref[:, lanes], write_low, 1, 1)
        read_sum = read_sum + dot(delta_end_ref[:, lanes], write_high, 1, 1)
    work_ref[:, half : half + STATE] = write_sum
    work_ref[:, half + STATE :] = read_sum
    tokens = mine_ref.shape[0]
    mine_ref[...] = work_ref[pl.ds(pl.multiple_of(core_ref[0] * tokens, tokens), tokens), :]
    send_ref[...] = work_ref[
        pl.ds(pl.multiple_of((1 - core_ref[0]) * tokens, tokens), tokens), :
    ].astype(bf16)


def tail(core, back, write, value_start, value_end, delta_start, delta_end, fades, base):
    rows, width = base.shape
    vmem = pl.BlockSpec(memory_space=pltpu.VMEM)
    return pl.pallas_call(
        tail_kernel,
        in_specs=[pl.BlockSpec(memory_space=pltpu.SMEM)] + [vmem] * 9,
        out_shape=(
            jax.ShapeDtypeStruct((rows // 2, width), f32),
            jax.ShapeDtypeStruct((rows // 2, width), bf16),
        ),
        scratch_shapes=[pltpu.VMEM((rows, width), f32)],
    )(core.reshape(1), back, write, value_start, value_end, delta_start, delta_end, *fades, base)


def to_message(low, high):
    def cut(a):
        n, w = a.shape
        return a.astype(bf16).reshape(n // 8, 8, w // 128, 128).transpose(2, 0, 1, 3)

    both = jnp.stack([cut(low), cut(high)], axis=2)
    return both.reshape(-1, 16, 128)


def on_device(
    layer_input,
    cotangent,
    routes,
    route_weight,
    gate_weight,
    up_weight,
    down_weight,
    heads_value,
    output_gate,
    mixer_saved,
    proj_weight,
    state_write,
    state_read,
    decay_rate,
):
    core = lax.axis_index(CORE)
    tp = lax.axis_index(TP)
    first = core == 0
    tokens, width = layer_input.shape
    chips = lax.axis_size(CHIPS)
    experts = 2 * chips
    cap = max(2, 3 * tokens * routes.shape[1] // (2 * experts))
    rows = 2 * cap
    n_tp = lax.axis_size(TP)
    heads = decay_rate.shape[1]
    half_heads = heads // 2
    half = heads_value.shape[1] // 2

    def ordered(mine, other, axis=0):
        return jnp.concatenate(
            [jnp.where(first, mine, other), jnp.where(first, other, mine)], axis=axis
        )

    def halves(a):
        left, right = a[:, : a.shape[1] // 2], a[:, a.shape[1] // 2 :]
        return jnp.where(first, left, right), jnp.where(first, right, left)

    small = jnp.concatenate([routes.astype(f32), route_weight, decay_rate], axis=1)
    small_other = swap(small)
    input_other = swap(layer_input)
    cotangent_other = swap(cotangent)

    routes_row = jnp.concatenate([routes.T, small_other[:, 0:2].T.astype(jnp.int32)], axis=1)
    weight_row = jnp.concatenate([route_weight.T, small_other[:, 2:4].T], axis=1)
    count = 2 * tokens
    token_row = lax.broadcasted_iota(jnp.int32, (1, count), 1)
    source_row = (token_row >= tokens).astype(jnp.int32)
    expert_col = lax.broadcasted_iota(jnp.int32, (experts, count), 0)
    named = [expert_col == routes_row[k : k + 1] for k in range(2)]
    named_any = (named[0] | named[1]).astype(bf16)
    earlier = lax.broadcasted_iota(jnp.int32, (count, count), 0)
    later = lax.broadcasted_iota(jnp.int32, (count, count), 1)
    before_mask = ((earlier < later) & ((earlier < tokens) == (later < tokens))).astype(bf16)
    before = dot(named_any, before_mask)
    place = []
    for k in range(2):
        rank = jnp.sum(jnp.where(named[k], before, 0.0), axis=0, keepdims=True).astype(jnp.int32)
        expert = routes_row[k : k + 1]
        here = (expert & 1) == core
        place.append(
            (jnp.where(here, expert >> 1, -1), source_row * cap + rank)
        )
    out_col = lax.broadcasted_iota(jnp.int32, (chips * 2 * rows, 2 * count), 0)
    pick = None
    scale = None
    for k in range(2):
        chip, inner = place[k]
        spot = jnp.where(chip < 0, -1, chip * (2 * rows) + inner)
        spots = jnp.concatenate([spot, jnp.where(spot < 0, -1, spot + rows)], axis=1)
        factor = jnp.concatenate([jnp.ones_like(weight_row[k : k + 1]), weight_row[k : k + 1]], axis=1)
        hit = out_col == spots
        part = jnp.where(hit, factor, 0.0)
        pick = hit if pick is None else pick | hit
        scale = part if scale is None else scale + part
    scale = jnp.sum(scale, axis=1, keepdims=True)
    stacked = jnp.concatenate([layer_input, input_other, cotangent, cotangent_other], axis=0)
    sent = (dot(pick.astype(bf16), stacked) * scale).astype(bf16)
    later_inputs = (gate_weight, up_weight, down_weight, heads_value, output_gate, mixer_saved)
    later_inputs += (proj_weight, state_write, state_read, decay_rate, small_other)
    sent, later_inputs = lax.optimization_barrier((sent, later_inputs))
    gate_weight, up_weight, down_weight, heads_value, output_gate, mixer_saved = later_inputs[:6]
    proj_weight, state_write, state_read, decay_rate, small_other = later_inputs[6:]

    back_col = lax.broadcasted_iota(jnp.int32, (chips * rows, count), 0)
    back = None
    for k in range(2):
        chip, inner = place[k]
        hit = back_col == jnp.where(chip < 0, -1, chip * rows + inner)
        back = hit if back is None else back | hit
    back = back.astype(bf16)

    active_gate, slope_gate = silu_parts(output_gate.astype(f32))
    saved = mixer_saved.astype(f32)
    gated = (saved * active_gate).astype(bf16)
    value_mine, value_send = halves(heads_value)
    gated_mine, gated_send = halves(gated)
    side = jnp.concatenate([value_send, gated_send, state_write, state_read], axis=1)
    side_other = swap(side)
    value = ordered(value_mine, side_other[:, :half])
    gated_all = jnp.concatenate([gated_mine, side_other[:, half : 2 * half]], axis=0)
    write = ordered(state_write, side_other[:, 2 * half : 2 * half + STATE])
    read = ordered(state_read, side_other[:, 2 * half + STATE :])
    rates = ordered(halves(decay_rate)[0], halves(small_other[:, 4:])[0])
    cumul = jnp.cumsum(rates, axis=0)
    spread = (
        lax.broadcasted_iota(jnp.int32, (half_heads, half), 1) // HEAD_DIM
        == lax.broadcasted_iota(jnp.int32, (half_heads, half), 0)
    ).astype(f32)
    cumul_wide = jnp.dot(cumul, spread, precision=lax.Precision.HIGHEST)
    total_wide = cumul_wide[-1:]
    fade_end = jnp.exp(cumul_wide - total_wide)
    fade_start = jnp.exp(-cumul_wide)
    value_f = value.astype(f32)
    value_end = (value_f * fade_end).astype(bf16)
    value_start = (value_f * fade_start).astype(bf16)
    write_states = to_message(dot(write, value_end, 0, 0), dot(write, value_start, 0, 0))
    total_high = lax.reduce_precision(total_wide, 8, 7)
    total_rows = jnp.concatenate(
        [total_high, total_wide - total_high, jnp.zeros((6, half), f32)], axis=0
    ).astype(bf16)
    total_rows = jnp.broadcast_to(
        total_rows.reshape(8, half // 128, 1, 128).transpose(1, 2, 0, 3),
        (half // 128, STATE // 8, 8, 128),
    ).reshape(-1, 8, 128)
    quarter = width

    def rolled(a):
        parts = a.reshape(n_tp, quarter, a.shape[1])
        return [
            lax.dynamic_index_in_dim(parts, (tp + i) & (n_tp - 1), 0, keepdims=False)
            for i in range(n_tp)
        ]

    def unrolled(parts):
        stack = jnp.stack(parts)
        return [
            lax.dynamic_index_in_dim(stack, (k + n_tp - tp) & (n_tp - 1), 0, keepdims=False)
            for k in range(n_tp)
        ]

    gate_up = [
        jnp.concatenate(pair, axis=1) for pair in zip(rolled(gate_weight[0]), rolled(up_weight[0]))
    ]
    down = [
        lax.dynamic_slice_in_dim(down_weight[0], ((tp + i) & (n_tp - 1)) * quarter, quarter, 1)
        for i in range(n_tp)
    ]
    proj = rolled(proj_weight)
    hid = gate_weight.shape[2]
    slots = chips * rows

    out_row = lax.broadcasted_iota(jnp.int32, (2 * slots, 2 * slots), 0)
    in_row = lax.broadcasted_iota(jnp.int32, (2 * slots, 2 * slots), 1)
    kind = (out_row >= slots).astype(jnp.int32)
    slot = out_row - kind * slots
    sort_rows = (slot + slot // rows * rows + kind * rows == in_row).astype(bf16)
    sort_rows, sent = lax.optimization_barrier((sort_rows, sent))
    received = exchange(sent.reshape(chips, 2 * rows, width)).reshape(2 * slots, width)
    sorted_rows = dot(sort_rows, received).astype(bf16)
    from_low = ring(sorted_rows, 1)
    from_up = ring(sorted_rows, -1)
    input_far = ring(from_low[:slots], 1)
    cotangent_far = ring(from_up[slots:], -1)
    input_parts = [sorted_rows[:slots], from_up[:slots], input_far, from_low[:slots]]
    cotangent_parts = [sorted_rows[slots:], from_up[slots:], cotangent_far, from_low[slots:]]
    order = (0, 1, 3, 2)
    pre = sum(dot(input_parts[i], gate_up[i]) for i in order)
    hidden_grad = sum(dot(cotangent_parts[i], down[i], 1, 1) for i in order)
    pre_gate, pre_up = pre[:, :hid], pre[:, hid:]
    active, slope = silu_parts(pre_gate)
    hidden = (active * pre_up).astype(bf16)
    deltas = jnp.concatenate(
        [(hidden_grad * pre_up * slope).astype(bf16), (hidden_grad * active).astype(bf16)], axis=1
    )
    ready = (write, read, value, gated_all, cumul, fade_end, fade_start, value_end, value_start)
    ready += (write_states, total_rows)
    deltas, ready = lax.optimization_barrier((deltas, ready))
    write, read, value, gated_all, cumul, fade_end, fade_start, value_end, value_start = ready[:9]
    write_states, total_rows = ready[9:]
    partial = [dot(deltas, gate_up[i], 1, 1).astype(bf16) for i in range(n_tp)]
    returned = ring_reduce(partial, TP).astype(bf16)
    returned, deltas, hidden = lax.optimization_barrier((returned, deltas, hidden))
    arrived = exchange(returned.reshape(chips, rows, width)).reshape(slots, width)

    both_grad = unrolled([dot(input_parts[i], deltas, 0, 0).astype(bf16) for i in range(n_tp)])
    gate_grad = jnp.concatenate([a[:, :hid] for a in both_grad], axis=0)[None]
    up_grad = jnp.concatenate([a[:, hid:] for a in both_grad], axis=0)[None]
    down_grad = jnp.concatenate(
        unrolled([dot(hidden, cotangent_parts[i], 0, 0).astype(bf16) for i in range(n_tp)]), axis=1
    )[None]

    summed = dot(back, arrived, 0, 0)
    summed_other = swap(summed[tokens:].astype(bf16)).astype(f32)
    layer_grad = (cotangent.astype(f32) + summed[:tokens] + summed_other).astype(bf16)
    grads = [layer_grad, ring(layer_grad, -1), ring(layer_grad, 2), ring(layer_grad, 1)]
    out_delta = sum(dot(grads[i], proj[i]) for i in (0, 1, 3, 2)).astype(bf16).astype(f32)
    outgate_grad = (out_delta * saved * slope_gate).astype(bf16)
    mixer_delta = (out_delta * active_gate).astype(bf16)
    delta_mine, delta_send = halves(mixer_delta)
    delta = ordered(delta_mine, swap(delta_send))
    delta_f = delta.astype(f32)
    delta_end = (delta_f * fade_end).astype(bf16)
    delta_start = (delta_f * fade_start).astype(bf16)
    read_states = to_message(dot(read, delta_end, 0, 0), dot(read, delta_start, 0, 0))
    states_got = exchange(jnp.concatenate([read_states, write_states, total_rows], axis=1))

    grad_mine = jnp.concatenate(grads, axis=1)
    grad_all = jnp.concatenate([grad_mine, swap(grad_mine)], axis=0)
    proj_part = dot(grad_all, gated_all, 0, 0).astype(bf16)
    deep, wide = lax.axis_size(SP[0]), lax.axis_size(SP[1])
    block = proj_part.shape[0] // chips
    across = lax.axis_index(SP[1])
    proj_part = jnp.stack(unrolled([
        proj_part[i * quarter : (i + 1) * quarter].reshape(deep // n_tp, wide, block, half)
        for i in range(n_tp)
    ]))
    proj_sum = ring_reduce(
        [
            lax.dynamic_index_in_dim(
                proj_part, (across + i) & (wide - 1), 2, keepdims=False
            ).reshape(deep, block, half)
            for i in range(wide)
        ],
        SP[1],
    )
    scanned = scan_chunks(states_got)
    states_back = exchange(scanned)
    depth = lax.axis_index(SP[0])
    gap = deep // 2
    while gap:
        upper = (depth & gap) != 0
        below, above = proj_sum[:gap], proj_sum[gap:]
        away = jnp.where(upper, below, above).astype(bf16)
        got = lax.ppermute(away, SP[0], [(i, i ^ gap) for i in range(deep)])
        proj_sum = jnp.where(upper, above, below) + got.astype(f32)
        gap //= 2
    proj_sum = proj_sum[0]
    top, bottom = proj_sum[: block // 2], proj_sum[block // 2 :]
    proj_mine = jnp.where(first, top, bottom)
    proj_grad = ordered(proj_mine, swap(jnp.where(first, bottom, top)), axis=1)

    cumul_row = cumul.T
    common = dot(read, write, 1, 1)
    score = None
    value_parts = []
    for h in range(half_heads):
        mix = jnp.exp(-jnp.abs(cumul[:, h : h + 1] - cumul_row[h : h + 1]))
        lanes = slice(h * HEAD_DIM, (h + 1) * HEAD_DIM)
        match = dot(delta[:, lanes], value[:, lanes], 1, 1) * mix
        score = match if score is None else score + match
        value_parts.append(dot((mix * common).astype(bf16), delta[:, lanes], 0, 0))
    score = score.astype(bf16)
    base = jnp.concatenate(value_parts + [dot(score, read, 0, 0), dot(score, write)], axis=1)
    outs_mine, outs_send = tail(
        core,
        states_back,
        write,
        value_start,
        value_end,
        delta_start,
        delta_end,
        (fade_start, fade_end),
        base,
    )
    outs_got = swap(outs_send)
    value_out = ordered(outs_mine[:, :half].astype(bf16), outs_got[:, :half], axis=1)
    sums = (outs_mine[:, half:] + outs_got[:, half:].astype(f32)).astype(bf16)
    return (
        gate_grad,
        up_grad,
        down_grad,
        proj_grad,
        value_out,
        sums[:, :STATE],
        sums[:, STATE:],
        outgate_grad,
    )


def solution(mesh):
    split = Mesh(mesh.devices.reshape(8, 4, 2, mesh.shape["tp"]), SP + (TP,))
    placed = (
        P(SP, TP),
        P(SP, TP),
        P(SP, None),
        P(SP, None),
        P(SP, None, TP),
        P(SP, None, TP),
        P(SP, TP, None),
        P(SP, TP),
        P(SP, TP),
        P(SP, TP),
        P(None, TP),
        P(SP, TP),
        P(SP, TP),
        P(SP, TP),
    )

    return jax.shard_map(
        on_device,
        mesh=split,
        in_specs=placed,
        out_specs=(
            P(SP, None, TP),
            P(SP, None, TP),
            P(SP, TP, None),
            P(SP, TP),
            P(SP, TP),
            P(SP, TP),
            P(SP, TP),
            P(SP, TP),
        ),
        check_vma=False,
    )
```

```python
import jax
import jax.numpy as jnp
from jax import lax
from jax.experimental import pallas as pl
from jax.experimental.pallas import tpu as pltpu
from jax.sharding import Mesh
from jax.sharding import PartitionSpec as P


HEAD_DIM = 64
STATE = 128
SP = ("sp_0", "sp_1", "sp_2")
CHIPS = ("sp_0", "sp_1")
CORE = "sp_2"
TP = "tp"

f32 = jnp.float32
bf16 = jnp.bfloat16


def dot(a, b, ca=1, cb=0):
    return lax.dot_general(a, b, (((ca,), (cb,)), ((), ())), preferred_element_type=f32)


def swap(x):
    return lax.ppermute(x, CORE, [(0, 1), (1, 0)])


def ring(x, shift, axis=TP):
    n = lax.axis_size(axis)
    return lax.ppermute(x, axis, [(i, (i + shift) % n) for i in range(n)])


def ring_reduce(parts, axis):
    own, right, far, left = parts
    opposite = ring(far, 2, axis)
    low = ring(right, 1, axis)
    up = ring(left, -1, axis)
    return own.astype(f32) + low.astype(f32) + up.astype(f32) + opposite.astype(f32)


def exchange(x):
    return lax.all_to_all(x, CHIPS, split_axis=0, concat_axis=0, tiled=True)


def silu_parts(value):
    sigma = jax.nn.sigmoid(value)
    return (value * sigma, sigma * (1.0 + value * (1.0 - sigma)))


def route_kernel(
    core_ref, mine_ref, other_ref, tokens_ref, tokens_other_ref, sent_ref, spot_ref
):
    tokens = tokens_ref.shape[0] // 2
    count = 2 * tokens
    total = sent_ref.shape[0]
    rows = spot_ref.shape[0] + 4
    cap = rows // 2
    experts = total // rows
    core = core_ref[0]
    table = jnp.concatenate([mine_ref[...], other_ref[...]], axis=1)
    ids = table[0:2].astype(jnp.int32)
    source = (lax.broadcasted_iota(jnp.int32, (1, count), 1) >= tokens).astype(jnp.int32)
    expert_col = lax.broadcasted_iota(jnp.int32, (experts, count), 0)
    named = [expert_col == ids[k : k + 1] for k in range(2)]
    named_any = jnp.where(named[0] | named[1], 1.0, 0.0).astype(bf16)
    earlier = lax.broadcasted_iota(jnp.int32, (count, count), 0)
    later = lax.broadcasted_iota(jnp.int32, (count, count), 1)
    ahead = jnp.where((earlier < later) & ((earlier >= tokens) | (later < tokens)), 1.0, 0.0)
    before = dot(named_any, ahead.astype(bf16))
    spots = []
    factors = []
    for k in range(2):
        rank = jnp.sum(jnp.where(named[k], before, 0.0), axis=0, keepdims=True).astype(jnp.int32)
        expert = ids[k : k + 1]
        spot = jnp.where(
            (expert & 1) == core, (expert >> 1) * (2 * rows) + source * cap + rank, -1
        )
        spot_ref[k : k + 1, :] = spot
        spots.append(jnp.concatenate([spot, jnp.where(spot < 0, -1, spot + rows)], axis=1))
        weight = table[2 + k : 3 + k]
        factors.append(jnp.concatenate([jnp.ones_like(weight), weight], axis=1))
    x_all = jnp.concatenate([tokens_ref[:tokens], tokens_other_ref[:tokens]], axis=0)
    c_all = jnp.concatenate([tokens_ref[tokens:], tokens_other_ref[tokens:]], axis=0)
    step = 64

    def block(i, carry):
        row = lax.broadcasted_iota(jnp.int32, (step, 2 * count), 0) + i * step
        hits = [row == spots[k] for k in range(2)]
        scale = jnp.sum(
            jnp.where(hits[0], factors[0], 0.0) + jnp.where(hits[1], factors[1], 0.0),
            axis=1,
            keepdims=True,
        )
        pick = jnp.where(hits[0] | hits[1], 1.0, 0.0).astype(bf16)
        made = dot(pick[:, :count], x_all) + dot(pick[:, count:], c_all)
        sent_ref[pl.ds(pl.multiple_of(i * step, step), step), :] = (made * scale).astype(bf16)
        return carry

    lax.fori_loop(0, total // step, block, 0)


def route(core, mine, other, both, both_other, chips, rows):
    vmem = pl.BlockSpec(memory_space=pltpu.VMEM)
    return pl.pallas_call(
        route_kernel,
        in_specs=[pl.BlockSpec(memory_space=pltpu.SMEM)] + [vmem] * 4,
        out_shape=(
            jax.ShapeDtypeStruct((chips * 2 * rows, both.shape[1]), bf16),
            jax.ShapeDtypeStruct((rows - 4, both.shape[0]), jnp.int32),
        ),
    )(core.reshape(1), mine, other, both, both_other)


def join_kernel(core_ref, mine_ref, got_ref, value_ref, write_ref, read_ref):
    half = value_ref.shape[1] // 2
    lead = core_ref[0] == 0
    mine = mine_ref[...]
    got = got_ref[...].astype(f32)
    value_ref[:, :half] = jnp.where(lead, mine[:, :half], got[:, :half]).astype(bf16)
    value_ref[:, half:] = jnp.where(lead, got[:, :half], mine[:, :half]).astype(bf16)
    sums = (mine[:, half:] + got[:, half:]).astype(bf16)
    write_ref[...] = sums[:, :STATE]
    read_ref[...] = sums[:, STATE:]


def join(core, mine, got):
    rows, width = mine.shape
    vmem = pl.BlockSpec(memory_space=pltpu.VMEM)
    narrow = jax.ShapeDtypeStruct((rows, STATE), bf16)
    return pl.pallas_call(
        join_kernel,
        in_specs=[pl.BlockSpec(memory_space=pltpu.SMEM), vmem, vmem],
        out_shape=(jax.ShapeDtypeStruct((rows, 2 * (width - 2 * STATE)), bf16), narrow, narrow),
    )(core.reshape(1), mine, got)


def scan_kernel(msg_ref, out_ref, work_ref):
    chunks, height, _ = out_ref.shape
    work_ref[...] = msg_ref[...].astype(f32)
    fades = [
        jnp.exp(-(work_ref[k, height : height + 1, :] + work_ref[k, height + 1 : height + 2, :]))
        for k in range(chunks)
    ]
    states = [jnp.zeros((8, 128), f32)] * (height // 8)
    for i in range(chunks):
        for s in range(height // 8):
            k = i if s % 2 == 0 else chunks - 1 - i
            rows = slice(s * 8, s * 8 + 8)
            own = work_ref[k, rows, :]
            work_ref[k, rows, :] = states[s]
            states[s] = states[s] * fades[k] + own
    out_ref[...] = work_ref[:, :height, :].astype(bf16)


def scan_chunks(msg):
    chunks, height, lanes = msg.shape
    return pl.pallas_call(
        scan_kernel,
        out_shape=jax.ShapeDtypeStruct((chunks, height - 8, lanes), bf16),
        scratch_shapes=[pltpu.VMEM(msg.shape, f32)],
    )(msg)


def tail_kernel(
    core_ref,
    back_ref,
    write_ref,
    value_start_ref,
    value_end_ref,
    delta_start_ref,
    delta_end_ref,
    fade_start_ref,
    fade_end_ref,
    base_ref,
    mine_ref,
    send_ref,
    work_ref,
):
    blocks = value_start_ref.shape[1] // 128
    steps = back_ref.shape[0] // blocks
    half = blocks * 128
    write = write_ref[...]
    write_sum = base_ref[:, half : half + STATE]
    read_sum = base_ref[:, half + STATE :]
    for q in range(blocks):
        states = back_ref[q * steps : (q + 1) * steps].astype(f32)
        read_low, read_high, write_low, write_high = (
            states[:, 8 * i : 8 * i + 8, :].reshape(STATE, 128).astype(bf16) for i in range(4)
        )
        lanes = slice(q * 128, (q + 1) * 128)
        work_ref[:, lanes] = (
            base_ref[:, lanes]
            + dot(write, read_low) * fade_start_ref[:, lanes]
            + dot(write, read_high) * fade_end_ref[:, lanes]
        )
        write_sum = write_sum + dot(value_start_ref[:, lanes], read_low, 1, 1)
        write_sum = write_sum + dot(value_end_ref[:, lanes], read_high, 1, 1)
        read_sum = read_sum + dot(delta_start_ref[:, lanes], write_low, 1, 1)
        read_sum = read_sum + dot(delta_end_ref[:, lanes], write_high, 1, 1)
    work_ref[:, half : half + STATE] = write_sum
    work_ref[:, half + STATE :] = read_sum
    tokens = mine_ref.shape[0]
    mine_ref[...] = work_ref[pl.ds(pl.multiple_of(core_ref[0] * tokens, tokens), tokens), :]
    send_ref[...] = work_ref[
        pl.ds(pl.multiple_of((1 - core_ref[0]) * tokens, tokens), tokens), :
    ].astype(bf16)


def tail(core, back, write, value_start, value_end, delta_start, delta_end, fades, base):
    rows, width = base.shape
    vmem = pl.BlockSpec(memory_space=pltpu.VMEM)
    return pl.pallas_call(
        tail_kernel,
        in_specs=[pl.BlockSpec(memory_space=pltpu.SMEM)] + [vmem] * 9,
        out_shape=(
            jax.ShapeDtypeStruct((rows // 2, width), f32),
            jax.ShapeDtypeStruct((rows // 2, width), bf16),
        ),
        scratch_shapes=[pltpu.VMEM((rows, width), f32)],
    )(core.reshape(1), back, write, value_start, value_end, delta_start, delta_end, *fades, base)


def to_message(low, high):
    def cut(a):
        n, w = a.shape
        return a.astype(bf16).reshape(n // 8, 8, w // 128, 128).transpose(2, 0, 1, 3)

    both = jnp.stack([cut(low), cut(high)], axis=2)
    return both.reshape(-1, 16, 128)


def on_device(
    layer_input,
    cotangent,
    routes,
    route_weight,
    gate_weight,
    up_weight,
    down_weight,
    heads_value,
    output_gate,
    mixer_saved,
    proj_weight,
    state_write,
    state_read,
    decay_rate,
):
    core = lax.axis_index(CORE)
    tp = lax.axis_index(TP)
    first = core == 0
    tokens, width = layer_input.shape
    chips = lax.axis_size(CHIPS)
    experts = 2 * chips
    cap = max(2, 3 * tokens * routes.shape[1] // (2 * experts))
    rows = 2 * cap
    n_tp = lax.axis_size(TP)
    heads = decay_rate.shape[1]
    half_heads = heads // 2
    half = heads_value.shape[1] // 2

    def ordered(mine, other, axis=0):
        return jnp.concatenate(
            [jnp.where(first, mine, other), jnp.where(first, other, mine)], axis=axis
        )

    def halves(a):
        left, right = a[:, : a.shape[1] // 2], a[:, a.shape[1] // 2 :]
        return jnp.where(first, left, right), jnp.where(first, right, left)

    small = jnp.concatenate([routes.T.astype(f32), route_weight.T, decay_rate.T], axis=0)
    small_other = swap(small)
    both = jnp.concatenate([layer_input, cotangent], axis=0)
    sent, spot = route(core, small, small_other, both, swap(both), chips, rows)
    later_inputs = (gate_weight, up_weight, down_weight, heads_value, output_gate, mixer_saved)
    later_inputs += (proj_weight, state_write, state_read, small, small_other)
    sent, later_inputs = lax.optimization_barrier((sent, later_inputs))
    gate_weight, up_weight, down_weight, heads_value, output_gate, mixer_saved = later_inputs[:6]
    proj_weight, state_write, state_read, small, small_other = later_inputs[6:]

    spot_row = lax.broadcasted_iota(jnp.int32, (chips * 2 * rows, 2 * tokens), 0)
    back = [
        sum(
            jnp.where((spot[k : k + 1] >= 0) & (spot_row == spot[k : k + 1] + j * rows), 1.0, 0.0)
            for k in range(2)
        ).astype(bf16)
        for j in range(2)
    ]

    active_gate, slope_gate = silu_parts(output_gate.astype(f32))
    saved = mixer_saved.astype(f32)
    gated = (saved * active_gate).astype(bf16)
    value_mine, value_send = halves(heads_value)
    side = jnp.concatenate([value_send, state_write, state_read, gated], axis=1)
    side_other = swap(side)
    slots = chips * rows
    out_row = lax.broadcasted_iota(jnp.int32, (slots, 2 * slots), 0)
    in_row = lax.broadcasted_iota(jnp.int32, (slots, 2 * slots), 1)
    origin = out_row + out_row // rows * rows
    sort_rows = [(origin + j * rows == in_row).astype(bf16) for j in range(2)]
    place = lax.broadcasted_iota(jnp.int32, (2 * slots, slots), 0)
    column = lax.broadcasted_iota(jnp.int32, (2 * slots, slots), 1)
    target = column + column // rows * rows
    spread_rows = [
        (place == target + j * rows).astype(bf16) for j in range(2)
    ]
    maps = (sort_rows, spread_rows, back)
    side_other, small, small_other, maps = lax.optimization_barrier(
        (side_other, small, small_other, maps)
    )
    sort_rows, spread_rows, back = maps
    value = ordered(value_mine, side_other[:, :half])
    gated_all = jnp.concatenate([gated, side_other[:, half + 2 * STATE :]], axis=0)
    write = ordered(state_write, side_other[:, half : half + STATE])
    read = ordered(state_read, side_other[:, half + STATE : half + 2 * STATE])
    rates = ordered(halves(small[4:].T)[0], halves(small_other[4:].T)[0])
    cumul = jnp.cumsum(rates, axis=0)
    spread = (
        lax.broadcasted_iota(jnp.int32, (half_heads, half), 1) // HEAD_DIM
        == lax.broadcasted_iota(jnp.int32, (half_heads, half), 0)
    ).astype(f32)
    cumul_wide = jnp.dot(cumul, spread, precision=lax.Precision.HIGHEST)
    total_wide = cumul_wide[-1:]
    fade_end = jnp.exp(cumul_wide - total_wide)
    fade_start = jnp.exp(-cumul_wide)
    value_f = value.astype(f32)
    value_end = (value_f * fade_end).astype(bf16)
    value_start = (value_f * fade_start).astype(bf16)
    write_states = to_message(dot(write, value_end, 0, 0), dot(write, value_start, 0, 0))
    total_high = lax.reduce_precision(total_wide, 8, 7)
    total_rows = jnp.concatenate(
        [total_high, total_wide - total_high, jnp.zeros((6, half), f32)], axis=0
    ).astype(bf16)
    total_rows = jnp.broadcast_to(
        total_rows.reshape(8, half // 128, 1, 128).transpose(1, 2, 0, 3),
        (half // 128, STATE // 8, 8, 128),
    ).reshape(-1, 8, 128)
    quarter = width

    def rolled(a):
        parts = a.reshape(n_tp, quarter, a.shape[1])
        return [
            lax.dynamic_index_in_dim(parts, (tp + i) & (n_tp - 1), 0, keepdims=False)
            for i in range(n_tp)
        ]

    def unrolled(parts):
        stack = jnp.stack(parts)
        return [
            lax.dynamic_index_in_dim(stack, (k + n_tp - tp) & (n_tp - 1), 0, keepdims=False)
            for k in range(n_tp)
        ]

    gate_up = [
        jnp.concatenate(pair, axis=1) for pair in zip(rolled(gate_weight[0]), rolled(up_weight[0]))
    ]
    down = [
        lax.dynamic_slice_in_dim(down_weight[0], ((tp + i) & (n_tp - 1)) * quarter, quarter, 1)
        for i in range(n_tp)
    ]
    proj = rolled(proj_weight)
    hid = gate_weight.shape[2]
    received = exchange(sent.reshape(chips, 2 * rows, width)).reshape(2 * slots, width)
    input_own, cotangent_own = (dot(a, received).astype(bf16) for a in sort_rows)
    input_low = ring(input_own, 1)
    cotangent_up = ring(cotangent_own, -1)
    input_up = ring(input_own, -1)
    cotangent_low = ring(cotangent_own, 1)
    input_far = ring(input_low, 1)
    cotangent_far = ring(cotangent_up, -1)
    input_parts = [input_own, input_up, input_far, input_low]
    cotangent_parts = [cotangent_own, cotangent_up, cotangent_far, cotangent_low]
    order = (0, 1, 3, 2)
    pre = sum(dot(input_parts[i], gate_up[i]) for i in order)
    hidden_grad = sum(dot(cotangent_parts[i], down[i], 1, 1) for i in order)
    pre_gate, pre_up = pre[:, :hid], pre[:, hid:]
    active, slope = silu_parts(pre_gate)
    hidden = (active * pre_up).astype(bf16)
    deltas = jnp.concatenate(
        [(hidden_grad * pre_up * slope).astype(bf16), (hidden_grad * active).astype(bf16)], axis=1
    )
    ready = (write, read, value, gated_all, cumul, fade_end, fade_start, value_end, value_start)
    ready += (write_states, total_rows)
    deltas, ready = lax.optimization_barrier((deltas, ready))
    write, read, value, gated_all, cumul, fade_end, fade_start, value_end, value_start = ready[:9]
    write_states, total_rows = ready[9:]
    partial = [dot(deltas, gate_up[i], 1, 1).astype(bf16) for i in range(n_tp)]
    returned = ring_reduce(partial, TP).astype(bf16)
    returned, deltas, hidden = lax.optimization_barrier((returned, deltas, hidden))
    cut = width // 2
    returned = dot(spread_rows[0], returned[:, :cut]) + dot(spread_rows[1], returned[:, cut:])
    arrived = exchange(returned.astype(bf16).reshape(chips, 2 * rows, cut))
    arrived = arrived.reshape(2 * slots, cut)

    both_grad = unrolled([dot(input_parts[i], deltas, 0, 0).astype(bf16) for i in range(n_tp)])
    gate_grad = jnp.concatenate([a[:, :hid] for a in both_grad], axis=0)[None]
    up_grad = jnp.concatenate([a[:, hid:] for a in both_grad], axis=0)[None]
    down_grad = jnp.concatenate(
        unrolled([dot(hidden, cotangent_parts[i], 0, 0).astype(bf16) for i in range(n_tp)]), axis=1
    )[None]

    arrived, gate_grad, up_grad, down_grad = lax.optimization_barrier(
        (arrived, gate_grad, up_grad, down_grad)
    )
    summed = jnp.concatenate([dot(back[0], arrived, 0, 0), dot(back[1], arrived, 0, 0)], axis=1)
    summed_other = swap(summed[tokens:].astype(bf16)).astype(f32)
    layer_grad = (cotangent.astype(f32) + summed[:tokens] + summed_other).astype(bf16)
    grads = [layer_grad, ring(layer_grad, -1), ring(layer_grad, 2), ring(layer_grad, 1)]
    out_delta = sum(dot(grads[i], proj[i]) for i in (0, 1, 3, 2)).astype(bf16).astype(f32)
    outgate_grad = (out_delta * saved * slope_gate).astype(bf16)
    mixer_delta = (out_delta * active_gate).astype(bf16)
    delta_mine, delta_send = halves(mixer_delta)
    delta = ordered(delta_mine, swap(delta_send))
    delta_f = delta.astype(f32)
    delta_end = (delta_f * fade_end).astype(bf16)
    delta_start = (delta_f * fade_start).astype(bf16)
    read_states = to_message(dot(read, delta_end, 0, 0), dot(read, delta_start, 0, 0))
    states_got = exchange(jnp.concatenate([read_states, write_states, total_rows], axis=1))

    grad_mine = jnp.concatenate(grads, axis=1)
    grad_all = jnp.concatenate([grad_mine, swap(grad_mine)], axis=0)
    proj_part = dot(grad_all, gated_all, 0, 0).astype(bf16)
    deep, wide = lax.axis_size(SP[0]), lax.axis_size(SP[1])
    block = proj_part.shape[0] // chips // 2
    across = lax.axis_index(SP[1])
    pieces = proj_part.reshape(n_tp, deep // n_tp, wide, 2, block, width)
    pieces = lax.dynamic_index_in_dim(pieces, core, 3, keepdims=False)
    proj_part = jnp.stack(unrolled([pieces[i] for i in range(n_tp)]))
    proj_sum = ring_reduce(
        [
            lax.dynamic_index_in_dim(
                proj_part, (across + i) & (wide - 1), 2, keepdims=False
            ).reshape(deep, block, width)
            for i in range(wide)
        ],
        SP[1],
    )
    scanned = scan_chunks(states_got)
    states_back = exchange(scanned)
    depth = lax.axis_index(SP[0])
    gap = 1
    while gap < deep:
        upper = (depth & gap) != 0
        pairs = proj_sum.reshape(-1, 2, block, width)
        below, above = pairs[:, 0], pairs[:, 1]
        away = jnp.where(upper, below, above).astype(bf16)
        got = lax.ppermute(away, SP[0], [(i, i ^ gap) for i in range(deep)])
        proj_sum = jnp.where(upper, above, below) + got.astype(f32)
        gap *= 2
    proj_grad = proj_sum[0]

    cumul_row = cumul.T
    common = dot(read, write, 1, 1)
    score = None
    value_parts = []
    for h in range(half_heads):
        mix = jnp.exp(-jnp.abs(cumul[:, h : h + 1] - cumul_row[h : h + 1]))
        lanes = slice(h * HEAD_DIM, (h + 1) * HEAD_DIM)
        match = dot(delta[:, lanes], value[:, lanes], 1, 1) * mix
        score = match if score is None else score + match
        value_parts.append(dot((mix * common).astype(bf16), delta[:, lanes], 0, 0))
    score = score.astype(bf16)
    base = jnp.concatenate(value_parts + [dot(score, read, 0, 0), dot(score, write)], axis=1)
    outs_mine, outs_send = tail(
        core,
        states_back,
        write,
        value_start,
        value_end,
        delta_start,
        delta_end,
        (fade_start, fade_end),
        base,
    )
    outs_got = swap(outs_send)
    value_out, write_out, read_out = join(core, outs_mine, outs_got)
    return (
        gate_grad,
        up_grad,
        down_grad,
        proj_grad,
        value_out,
        write_out,
        read_out,
        outgate_grad,
    )


def solution(mesh):
    split = Mesh(mesh.devices.reshape(8, 4, 2, mesh.shape["tp"]), SP + (TP,))
    placed = (
        P(SP, TP),
        P(SP, TP),
        P(SP, None),
        P(SP, None),
        P(SP, None, TP),
        P(SP, None, TP),
        P(SP, TP, None),
        P(SP, TP),
        P(SP, TP),
        P(SP, TP),
        P(None, TP),
        P(SP, TP),
        P(SP, TP),
        P(SP, TP),
    )

    return jax.shard_map(
        on_device,
        mesh=split,
        in_specs=placed,
        out_specs=(
            P(SP, None, TP),
            P(SP, None, TP),
            P(SP, TP, None),
            P(SP, TP),
            P(SP, TP),
            P(SP, TP),
            P(SP, TP),
            P(SP, TP),
        ),
        check_vma=False,
    )
```

```python
import jax
import jax.numpy as jnp
from jax import lax
from jax.experimental import pallas as pl
from jax.experimental.pallas import tpu as pltpu
from jax.sharding import Mesh
from jax.sharding import PartitionSpec as P


HEAD_DIM = 64
STATE = 128
SP = ("sp_0", "sp_1", "sp_2")
CHIPS = ("sp_0", "sp_1")
CORE = "sp_2"
TP = "tp"

f32 = jnp.float32
bf16 = jnp.bfloat16


def dot(a, b, ca=1, cb=0):
    return lax.dot_general(a, b, (((ca,), (cb,)), ((), ())), preferred_element_type=f32)


def swap(x):
    return lax.ppermute(x, CORE, [(0, 1), (1, 0)])


def ring(x, shift, axis=TP):
    n = lax.axis_size(axis)
    return lax.ppermute(x, axis, [(i, (i + shift) % n) for i in range(n)])


def ring_reduce(parts, axis):
    own, right, far, left = parts
    opposite = ring(far, 2, axis)
    low = ring(right, 1, axis)
    up = ring(left, -1, axis)
    return own.astype(f32) + low.astype(f32) + up.astype(f32) + opposite.astype(f32)


def exchange(x):
    return lax.all_to_all(x, CHIPS, split_axis=0, concat_axis=0, tiled=True)


def silu_parts(value):
    sigma = jax.nn.sigmoid(value)
    return (value * sigma, sigma * (1.0 + value * (1.0 - sigma)))


def route_kernel(
    core_ref, mine_ref, other_ref, x_ref, x_other_ref, c_ref, c_other_ref, sent_ref, spot_ref
):
    tokens = x_ref.shape[0]
    count = 2 * tokens
    total = sent_ref.shape[0]
    rows = spot_ref.shape[0] + 4
    cap = rows // 2
    experts = total // rows
    core = core_ref[0]
    table = jnp.concatenate([mine_ref[...], other_ref[...]], axis=1)
    ids = table[0:2].astype(jnp.int32)
    source = (lax.broadcasted_iota(jnp.int32, (1, count), 1) >= tokens).astype(jnp.int32)
    expert_col = lax.broadcasted_iota(jnp.int32, (experts, count), 0)
    named = [expert_col == ids[k : k + 1] for k in range(2)]
    named_any = jnp.where(named[0] | named[1], 1.0, 0.0).astype(bf16)
    earlier = lax.broadcasted_iota(jnp.int32, (count, count), 0)
    later = lax.broadcasted_iota(jnp.int32, (count, count), 1)
    ahead = jnp.where((earlier < later) & ((earlier >= tokens) | (later < tokens)), 1.0, 0.0)
    before = dot(named_any, ahead.astype(bf16))
    spots = []
    factors = []
    for k in range(2):
        rank = jnp.sum(jnp.where(named[k], before, 0.0), axis=0, keepdims=True).astype(jnp.int32)
        expert = ids[k : k + 1]
        spot = jnp.where(
            (expert & 1) == core, (expert >> 1) * (2 * rows) + source * cap + rank, -1
        )
        spot_ref[k : k + 1, :] = spot
        spots.append(jnp.concatenate([spot, jnp.where(spot < 0, -1, spot + rows)], axis=1))
        weight = table[2 + k : 3 + k]
        factors.append(jnp.concatenate([jnp.ones_like(weight), weight], axis=1))
    x_all = jnp.concatenate([x_ref[...], x_other_ref[...]], axis=0)
    c_all = jnp.concatenate([c_ref[...], c_other_ref[...]], axis=0)
    step = total // 4

    def block(i, carry):
        row = lax.broadcasted_iota(jnp.int32, (step, 2 * count), 0) + i * step
        hits = [row == spots[k] for k in range(2)]
        scale = jnp.sum(
            jnp.where(hits[0], factors[0], 0.0) + jnp.where(hits[1], factors[1], 0.0),
            axis=1,
            keepdims=True,
        )
        pick = jnp.where(hits[0] | hits[1], 1.0, 0.0).astype(bf16)
        made = dot(pick[:, :count], x_all) + dot(pick[:, count:], c_all)
        sent_ref[pl.ds(pl.multiple_of(i * step, step), step), :] = (made * scale).astype(bf16)
        return carry

    lax.fori_loop(0, total // step, block, 0)


def route(core, mine, other, x, x_other, c, c_other, chips, rows):
    vmem = pl.BlockSpec(memory_space=pltpu.VMEM)
    return pl.pallas_call(
        route_kernel,
        in_specs=[pl.BlockSpec(memory_space=pltpu.SMEM)] + [vmem] * 6,
        out_shape=(
            jax.ShapeDtypeStruct((chips * 2 * rows, x.shape[1]), bf16),
            jax.ShapeDtypeStruct((rows - 4, 2 * x.shape[0]), jnp.int32),
        ),
    )(core.reshape(1), mine, other, x, x_other, c, c_other)


GROUP = 4
ROWS = 24


def split_kernel(got_ref, x_ref, c_ref):
    slots = x_ref.shape[0]
    part = x_ref.shape[0] // (got_ref.shape[0] // ROWS // GROUP)
    out_row = lax.broadcasted_iota(jnp.int32, (2 * part, 2 * part), 0)
    in_row = lax.broadcasted_iota(jnp.int32, (2 * part, 2 * part), 1)
    kind = (out_row >= part).astype(jnp.int32)
    slot = out_row - kind * part
    rows = part // GROUP
    chip = sum((slot >= k * rows).astype(jnp.int32) for k in range(1, GROUP))
    perm = jnp.where(slot + chip * rows + kind * rows == in_row, 1.0, 0.0).astype(bf16)

    def block(i, carry):
        start = pl.multiple_of(i * 2 * part, 2 * part)
        made = dot(perm, got_ref[pl.ds(start, 2 * part), :]).astype(bf16)
        place = pl.multiple_of(i * part, part)
        x_ref[pl.ds(place, part), :] = made[:part]
        c_ref[pl.ds(place, part), :] = made[part:]
        return carry

    lax.fori_loop(0, slots // part, block, 0)


def split(got):
    shape = jax.ShapeDtypeStruct((got.shape[0] // 2, got.shape[1]), bf16)
    return pl.pallas_call(split_kernel, out_shape=(shape, shape))(got)


def spread_kernel(own_ref, low_ref, up_ref, far_ref, sent_ref):
    slots, width = own_ref.shape
    cut = width // 2
    part = slots // (sent_ref.shape[0] // ROWS // GROUP)
    out_row = lax.broadcasted_iota(jnp.int32, (2 * part, part), 0)
    slot = lax.broadcasted_iota(jnp.int32, (2 * part, part), 1)
    rows = part // GROUP
    chip = sum((slot >= k * rows).astype(jnp.int32) for k in range(1, GROUP))
    perms = [
        jnp.where(slot + chip * rows + j * rows == out_row, 1.0, 0.0).astype(bf16)
        for j in range(2)
    ]

    def block(i, carry):
        here = pl.ds(pl.multiple_of(i * part, part), part)
        total = own_ref[here, :].astype(f32) + low_ref[here, :].astype(f32)
        total = total + up_ref[here, :].astype(f32) + far_ref[here, :].astype(f32)
        total = total.astype(bf16)
        made = dot(perms[0], total[:, :cut]) + dot(perms[1], total[:, cut:])
        start = pl.multiple_of(i * 2 * part, 2 * part)
        sent_ref[pl.ds(start, 2 * part), :] = made.astype(bf16)
        return carry

    lax.fori_loop(0, slots // part, block, 0)


def spread(own, low, up, far):
    shape = jax.ShapeDtypeStruct((2 * own.shape[0], own.shape[1] // 2), bf16)
    return pl.pallas_call(spread_kernel, out_shape=shape)(own, low, up, far)


def mix_kernel(delta_ref, value_ref, write_ref, read_ref, wide_ref, row_ref, base_ref):
    half = value_ref.shape[1]
    write = write_ref[...]
    read = read_ref[...]
    common = dot(write, read, 1, 1)
    score = None
    turned = None
    for h in range(half // HEAD_DIM):
        lanes = slice(h * HEAD_DIM, (h + 1) * HEAD_DIM)
        mix = jnp.exp(-jnp.abs(wide_ref[:, h * HEAD_DIM : h * HEAD_DIM + 1] - row_ref[h : h + 1, :]))
        delta = delta_ref[:, lanes]
        value = value_ref[:, lanes]
        base_ref[:, lanes] = dot((mix * common).astype(bf16), delta)
        here = dot(delta, value, 1, 1) * mix
        there = dot(value, delta, 1, 1) * mix
        score = here if score is None else score + here
        turned = there if turned is None else turned + there
    base_ref[:, half : half + STATE] = dot(turned.astype(bf16), read)
    base_ref[:, half + STATE :] = dot(score.astype(bf16), write)


def mix_chunk(delta, value, write, read, wide, row):
    shape = jax.ShapeDtypeStruct((value.shape[0], value.shape[1] + 2 * STATE), f32)
    return pl.pallas_call(mix_kernel, out_shape=shape)(delta, value, write, read, wide, row)


def join_kernel(core_ref, mine_ref, got_ref, value_ref, write_ref, read_ref):
    half = value_ref.shape[1] // 2
    lead = core_ref[0] == 0
    mine = mine_ref[...]
    got = got_ref[...].astype(f32)
    value_ref[:, :half] = jnp.where(lead, mine[:, :half], got[:, :half]).astype(bf16)
    value_ref[:, half:] = jnp.where(lead, got[:, :half], mine[:, :half]).astype(bf16)
    sums = (mine[:, half:] + got[:, half:]).astype(bf16)
    write_ref[...] = sums[:, :STATE]
    read_ref[...] = sums[:, STATE:]


def join(core, mine, got):
    rows, width = mine.shape
    vmem = pl.BlockSpec(memory_space=pltpu.VMEM)
    narrow = jax.ShapeDtypeStruct((rows, STATE), bf16)
    return pl.pallas_call(
        join_kernel,
        in_specs=[pl.BlockSpec(memory_space=pltpu.SMEM), vmem, vmem],
        out_shape=(jax.ShapeDtypeStruct((rows, 2 * (width - 2 * STATE)), bf16), narrow, narrow),
    )(core.reshape(1), mine, got)


def scan_kernel(msg_ref, out_ref, work_ref):
    chunks, height, _ = out_ref.shape
    work_ref[...] = msg_ref[...].astype(f32)
    fades = [
        jnp.exp(-(work_ref[k, height : height + 1, :] + work_ref[k, height + 1 : height + 2, :]))
        for k in range(chunks)
    ]
    states = [jnp.zeros((8, 128), f32)] * (height // 8)
    for i in range(chunks):
        for s in range(height // 8):
            k = i if s % 2 == 0 else chunks - 1 - i
            rows = slice(s * 8, s * 8 + 8)
            own = work_ref[k, rows, :]
            work_ref[k, rows, :] = states[s]
            states[s] = states[s] * fades[k] + own
    out_ref[...] = work_ref[:, :height, :].astype(bf16)


def scan_chunks(msg):
    chunks, height, lanes = msg.shape
    return pl.pallas_call(
        scan_kernel,
        out_shape=jax.ShapeDtypeStruct((chunks, height - 8, lanes), bf16),
        scratch_shapes=[pltpu.VMEM(msg.shape, f32)],
    )(msg)


def tail_kernel(
    core_ref,
    back_ref,
    write_ref,
    value_start_ref,
    value_end_ref,
    delta_start_ref,
    delta_end_ref,
    fade_start_ref,
    fade_end_ref,
    base_ref,
    mine_ref,
    send_ref,
    work_ref,
):
    blocks = value_start_ref.shape[1] // 128
    steps = back_ref.shape[0] // blocks
    half = blocks * 128
    write = write_ref[...]
    write_sum = base_ref[:, half : half + STATE]
    read_sum = base_ref[:, half + STATE :]
    for q in range(blocks):
        states = back_ref[q * steps : (q + 1) * steps].astype(f32)
        read_low, read_high, write_low, write_high = (
            states[:, 8 * i : 8 * i + 8, :].reshape(STATE, 128).astype(bf16) for i in range(4)
        )
        lanes = slice(q * 128, (q + 1) * 128)
        work_ref[:, lanes] = (
            base_ref[:, lanes]
            + dot(write, read_low) * fade_start_ref[:, lanes]
            + dot(write, read_high) * fade_end_ref[:, lanes]
        )
        write_sum = write_sum + dot(value_start_ref[:, lanes], read_low, 1, 1)
        write_sum = write_sum + dot(value_end_ref[:, lanes], read_high, 1, 1)
        read_sum = read_sum + dot(delta_start_ref[:, lanes], write_low, 1, 1)
        read_sum = read_sum + dot(delta_end_ref[:, lanes], write_high, 1, 1)
    work_ref[:, half : half + STATE] = write_sum
    work_ref[:, half + STATE :] = read_sum
    tokens = mine_ref.shape[0]
    mine_ref[...] = work_ref[pl.ds(pl.multiple_of(core_ref[0] * tokens, tokens), tokens), :]
    send_ref[...] = work_ref[
        pl.ds(pl.multiple_of((1 - core_ref[0]) * tokens, tokens), tokens), :
    ].astype(bf16)


def tail(core, back, write, value_start, value_end, delta_start, delta_end, fades, base):
    rows, width = base.shape
    vmem = pl.BlockSpec(memory_space=pltpu.VMEM)
    return pl.pallas_call(
        tail_kernel,
        in_specs=[pl.BlockSpec(memory_space=pltpu.SMEM)] + [vmem] * 9,
        out_shape=(
            jax.ShapeDtypeStruct((rows // 2, width), f32),
            jax.ShapeDtypeStruct((rows // 2, width), bf16),
        ),
        scratch_shapes=[pltpu.VMEM((rows, width), f32)],
    )(core.reshape(1), back, write, value_start, value_end, delta_start, delta_end, *fades, base)


def to_message(low, high):
    def cut(a):
        n, w = a.shape
        return a.astype(bf16).reshape(n // 8, 8, w // 128, 128).transpose(2, 0, 1, 3)

    both = jnp.stack([cut(low), cut(high)], axis=2)
    return both.reshape(-1, 16, 128)


def on_device(
    layer_input,
    cotangent,
    routes,
    route_weight,
    gate_weight,
    up_weight,
    down_weight,
    heads_value,
    output_gate,
    mixer_saved,
    proj_weight,
    state_write,
    state_read,
    decay_rate,
):
    core = lax.axis_index(CORE)
    tp = lax.axis_index(TP)
    first = core == 0
    tokens, width = layer_input.shape
    chips = lax.axis_size(CHIPS)
    experts = 2 * chips
    cap = max(2, 3 * tokens * routes.shape[1] // (2 * experts))
    rows = 2 * cap
    n_tp = lax.axis_size(TP)
    heads = decay_rate.shape[1]
    half_heads = heads // 2
    half = heads_value.shape[1] // 2

    def ordered(mine, other, axis=0):
        return jnp.concatenate(
            [jnp.where(first, mine, other), jnp.where(first, other, mine)], axis=axis
        )

    def halves(a):
        left, right = a[:, : a.shape[1] // 2], a[:, a.shape[1] // 2 :]
        return jnp.where(first, left, right), jnp.where(first, right, left)

    small = jnp.concatenate([routes.T.astype(f32), route_weight.T, decay_rate.T], axis=0)
    small_other = swap(small)
    input_other = swap(layer_input)
    cotangent_other = swap(cotangent)
    sent, spot = route(
        core,
        small,
        small_other,
        layer_input,
        input_other,
        cotangent,
        cotangent_other,
        chips,
        rows,
    )
    later_inputs = (gate_weight, up_weight, down_weight, heads_value, output_gate, mixer_saved)
    later_inputs += (proj_weight, state_write, state_read, small, small_other)
    sent, later_inputs = lax.optimization_barrier((sent, later_inputs))
    gate_weight, up_weight, down_weight, heads_value, output_gate, mixer_saved = later_inputs[:6]
    proj_weight, state_write, state_read, small, small_other = later_inputs[6:]

    spot_row = lax.broadcasted_iota(jnp.int32, (chips * 2 * rows, 2 * tokens), 0)
    back = [
        sum(
            jnp.where((spot[k : k + 1] >= 0) & (spot_row == spot[k : k + 1] + j * rows), 1.0, 0.0)
            for k in range(2)
        ).astype(bf16)
        for j in range(2)
    ]

    active_gate, slope_gate = silu_parts(output_gate.astype(f32))
    saved = mixer_saved.astype(f32)
    gated = (saved * active_gate).astype(bf16)
    value_mine, value_send = halves(heads_value)
    side = jnp.concatenate([value_send, state_write, state_read, gated], axis=1)
    side_other = swap(side)
    slots = chips * rows
    slots = chips * rows
    side_other, small, small_other, back = lax.optimization_barrier(
        (side_other, small, small_other, back)
    )
    value = ordered(value_mine, side_other[:, :half])
    gated_all = jnp.concatenate([gated, side_other[:, half + 2 * STATE :]], axis=0)
    write = ordered(state_write, side_other[:, half : half + STATE])
    read = ordered(state_read, side_other[:, half + STATE : half + 2 * STATE])
    rates = ordered(
        *(jnp.where(first, a[4 : 4 + half_heads], a[4 + half_heads :]) for a in (small, small_other)),
        axis=1,
    )
    cumul_row = jnp.cumsum(rates, axis=1)
    spread_heads = (
        lax.broadcasted_iota(jnp.int32, (half_heads, half), 1) // HEAD_DIM
        == lax.broadcasted_iota(jnp.int32, (half_heads, half), 0)
    ).astype(f32)
    cumul_wide = lax.dot_general(
        cumul_row,
        spread_heads,
        (((0,), (0,)), ((), ())),
        precision=lax.Precision.HIGHEST,
        preferred_element_type=f32,
    )
    total_wide = cumul_wide[-1:]
    fade_end = jnp.exp(cumul_wide - total_wide)
    fade_start = jnp.exp(-cumul_wide)
    value_f = value.astype(f32)
    value_end = (value_f * fade_end).astype(bf16)
    value_start = (value_f * fade_start).astype(bf16)
    write_states = to_message(dot(write, value_end, 0, 0), dot(write, value_start, 0, 0))
    total_high = lax.reduce_precision(total_wide, 8, 7)
    total_rows = jnp.concatenate(
        [total_high, total_wide - total_high, jnp.zeros((6, half), f32)], axis=0
    ).astype(bf16)
    total_rows = jnp.broadcast_to(
        total_rows.reshape(8, half // 128, 1, 128).transpose(1, 2, 0, 3),
        (half // 128, STATE // 8, 8, 128),
    ).reshape(-1, 8, 128)
    quarter = width

    def rolled(a):
        parts = a.reshape(n_tp, quarter, a.shape[1])
        return [
            lax.dynamic_index_in_dim(parts, (tp + i) & (n_tp - 1), 0, keepdims=False)
            for i in range(n_tp)
        ]

    def unrolled(parts):
        stack = jnp.stack(parts)
        return [
            lax.dynamic_index_in_dim(stack, (k + n_tp - tp) & (n_tp - 1), 0, keepdims=False)
            for k in range(n_tp)
        ]

    gate_up = [
        jnp.concatenate(pair, axis=1) for pair in zip(rolled(gate_weight[0]), rolled(up_weight[0]))
    ]
    down = [
        lax.dynamic_slice_in_dim(down_weight[0], ((tp + i) & (n_tp - 1)) * quarter, quarter, 1)
        for i in range(n_tp)
    ]
    proj = rolled(proj_weight)
    hid = gate_weight.shape[2]
    received = exchange(sent.reshape(chips, 2 * rows, width)).reshape(2 * slots, width)
    input_own, cotangent_own = split(received)
    input_low = ring(input_own, 1)
    cotangent_up = ring(cotangent_own, -1)
    input_up = ring(input_own, -1)
    cotangent_low = ring(cotangent_own, 1)
    input_far = ring(input_low, 1)
    cotangent_far = ring(cotangent_up, -1)
    input_parts = [input_own, input_up, input_far, input_low]
    cotangent_parts = [cotangent_own, cotangent_up, cotangent_far, cotangent_low]
    order = (0, 1, 3, 2)
    pre = sum(dot(input_parts[i], gate_up[i]) for i in order)
    hidden_grad = sum(dot(cotangent_parts[i], down[i], 1, 1) for i in order)
    pre_gate, pre_up = pre[:, :hid], pre[:, hid:]
    active, slope = silu_parts(pre_gate)
    hidden = (active * pre_up).astype(bf16)
    deltas = jnp.concatenate(
        [(hidden_grad * pre_up * slope).astype(bf16), (hidden_grad * active).astype(bf16)], axis=1
    )
    ready = (write, read, value, gated_all, fade_end, fade_start, value_end, value_start)
    ready += (write_states, total_rows, cumul_wide, cumul_row)
    deltas, ready = lax.optimization_barrier((deltas, ready))
    write, read, value, gated_all, fade_end, fade_start, value_end, value_start = ready[:8]
    write_states, total_rows, cumul_wide, cumul_row = ready[8:]
    partial = [dot(deltas, gate_up[i], 1, 1).astype(bf16) for i in range(n_tp)]
    own, right, far, left = partial
    opposite = ring(far, 2)
    returned = spread(own, ring(right, 1), ring(left, -1), opposite)
    returned, deltas, hidden = lax.optimization_barrier((returned, deltas, hidden))
    cut = width // 2
    arrived = exchange(returned.reshape(chips, 2 * rows, cut))
    arrived = arrived.reshape(2 * slots, cut)

    both_grad = unrolled([dot(input_parts[i], deltas, 0, 0).astype(bf16) for i in range(n_tp)])
    gate_grad = jnp.concatenate([a[:, :hid] for a in both_grad], axis=0)[None]
    up_grad = jnp.concatenate([a[:, hid:] for a in both_grad], axis=0)[None]
    down_grad = jnp.concatenate(
        unrolled([dot(hidden, cotangent_parts[i], 0, 0).astype(bf16) for i in range(n_tp)]), axis=1
    )[None]

    arrived, gate_grad, up_grad, down_grad = lax.optimization_barrier(
        (arrived, gate_grad, up_grad, down_grad)
    )
    summed = jnp.concatenate([dot(back[0], arrived, 0, 0), dot(back[1], arrived, 0, 0)], axis=1)
    summed_other = swap(summed[tokens:].astype(bf16)).astype(f32)
    layer_grad = (cotangent.astype(f32) + summed[:tokens] + summed_other).astype(bf16)
    grads = [layer_grad, ring(layer_grad, -1), ring(layer_grad, 2), ring(layer_grad, 1)]
    out_delta = sum(dot(grads[i], proj[i]) for i in (0, 1, 3, 2)).astype(bf16).astype(f32)
    outgate_grad = (out_delta * saved * slope_gate).astype(bf16)
    mixer_delta = (out_delta * active_gate).astype(bf16)
    delta_mine, delta_send = halves(mixer_delta)
    delta = ordered(delta_mine, swap(delta_send))
    delta_f = delta.astype(f32)
    delta_end = (delta_f * fade_end).astype(bf16)
    delta_start = (delta_f * fade_start).astype(bf16)
    read_states = to_message(dot(read, delta_end, 0, 0), dot(read, delta_start, 0, 0))
    states_got = exchange(jnp.concatenate([read_states, write_states, total_rows], axis=1))

    grad_mine = jnp.concatenate(grads, axis=1)
    grad_all = jnp.concatenate([grad_mine, swap(grad_mine)], axis=0)
    proj_part = dot(grad_all, gated_all, 0, 0).astype(bf16)
    deep, wide = lax.axis_size(SP[0]), lax.axis_size(SP[1])
    block = proj_part.shape[0] // chips // 2
    across = lax.axis_index(SP[1])
    pieces = proj_part.reshape(n_tp, deep // n_tp, wide, 2, block, width)
    pieces = lax.dynamic_index_in_dim(pieces, core, 3, keepdims=False)
    proj_part = jnp.stack(unrolled([pieces[i] for i in range(n_tp)]))
    proj_sum = ring_reduce(
        [
            lax.dynamic_index_in_dim(
                proj_part, (across + i) & (wide - 1), 2, keepdims=False
            ).reshape(deep, block, width)
            for i in range(wide)
        ],
        SP[1],
    )
    scanned = scan_chunks(states_got)
    states_back = exchange(scanned)
    depth = lax.axis_index(SP[0])
    gap = 1
    while gap < deep:
        upper = (depth & gap) != 0
        pairs = proj_sum.reshape(-1, 2, block, width)
        below, above = pairs[:, 0], pairs[:, 1]
        away = jnp.where(upper, below, above).astype(bf16)
        got = lax.ppermute(away, SP[0], [(i, i ^ gap) for i in range(deep)])
        proj_sum = jnp.where(upper, above, below) + got.astype(f32)
        gap *= 2
    proj_grad = proj_sum[0]

    base = mix_chunk(delta, value, write, read, cumul_wide, cumul_row)
    outs_mine, outs_send = tail(
        core,
        states_back,
        write,
        value_start,
        value_end,
        delta_start,
        delta_end,
        (fade_start, fade_end),
        base,
    )
    outs_got = swap(outs_send)
    value_out, write_out, read_out = join(core, outs_mine, outs_got)
    return (
        gate_grad,
        up_grad,
        down_grad,
        proj_grad,
        value_out,
        write_out,
        read_out,
        outgate_grad,
    )


def solution(mesh):
    split = Mesh(mesh.devices.reshape(8, 4, 2, mesh.shape["tp"]), SP + (TP,))
    placed = (
        P(SP, TP),
        P(SP, TP),
        P(SP, None),
        P(SP, None),
        P(SP, None, TP),
        P(SP, None, TP),
        P(SP, TP, None),
        P(SP, TP),
        P(SP, TP),
        P(SP, TP),
        P(None, TP),
        P(SP, TP),
        P(SP, TP),
        P(SP, TP),
    )

    return jax.shard_map(
        on_device,
        mesh=split,
        in_specs=placed,
        out_specs=(
            P(SP, None, TP),
            P(SP, None, TP),
            P(SP, TP, None),
            P(SP, TP),
            P(SP, TP),
            P(SP, TP),
            P(SP, TP),
            P(SP, TP),
        ),
        check_vma=False,
    )
```

```python
import jax
import jax.numpy as jnp
from jax import lax
from jax.experimental import pallas as pl
from jax.experimental.pallas import tpu as pltpu
from jax.sharding import Mesh
from jax.sharding import PartitionSpec as P


HEAD_DIM = 64
STATE = 128
SP = ("sp_0", "sp_1", "sp_2")
CHIPS = ("sp_0", "sp_1")
CORE = "sp_2"
TP = "tp"

f32 = jnp.float32
bf16 = jnp.bfloat16


def dot(a, b, ca=1, cb=0):
    return lax.dot_general(a, b, (((ca,), (cb,)), ((), ())), preferred_element_type=f32)


def swap(x):
    return lax.ppermute(x, CORE, [(0, 1), (1, 0)])


def ring(x, shift, axis=TP):
    n = lax.axis_size(axis)
    return lax.ppermute(x, axis, [(i, (i + shift) % n) for i in range(n)])


def ring_reduce(parts, axis):
    own, right, far, left = parts
    opposite = ring(far, 2, axis)
    low = ring(right, 1, axis)
    up = ring(left, -1, axis)
    return own.astype(f32) + low.astype(f32) + up.astype(f32) + opposite.astype(f32)


def exchange(x):
    return lax.all_to_all(x, CHIPS, split_axis=0, concat_axis=0, tiled=True)


def silu_parts(value):
    sigma = jax.nn.sigmoid(value)
    return (value * sigma, sigma * (1.0 + value * (1.0 - sigma)))


def route_kernel(
    core_ref, mine_ref, other_ref, x_ref, x_other_ref, c_ref, c_other_ref, sent_ref, spot_ref
):
    tokens = x_ref.shape[0]
    count = 2 * tokens
    total = sent_ref.shape[0]
    rows = spot_ref.shape[0] + 4
    cap = rows // 2
    experts = total // rows
    core = core_ref[0]
    table = jnp.concatenate([mine_ref[...], other_ref[...]], axis=1)
    ids = table[0:2].astype(jnp.int32)
    source = (lax.broadcasted_iota(jnp.int32, (1, count), 1) >= tokens).astype(jnp.int32)
    expert_col = lax.broadcasted_iota(jnp.int32, (experts, count), 0)
    named = [expert_col == ids[k : k + 1] for k in range(2)]
    named_any = jnp.where(named[0] | named[1], 1.0, 0.0).astype(bf16)
    earlier = lax.broadcasted_iota(jnp.int32, (count, count), 0)
    later = lax.broadcasted_iota(jnp.int32, (count, count), 1)
    ahead = jnp.where((earlier < later) & ((earlier >= tokens) | (later < tokens)), 1.0, 0.0)
    before = dot(named_any, ahead.astype(bf16))
    spots = []
    factors = []
    for k in range(2):
        rank = jnp.sum(jnp.where(named[k], before, 0.0), axis=0, keepdims=True).astype(jnp.int32)
        expert = ids[k : k + 1]
        spot = jnp.where(
            (expert & 1) == core, (expert >> 1) * (2 * rows) + source * cap + rank, -1
        )
        spot_ref[k : k + 1, :] = spot
        spots.append(jnp.concatenate([spot, jnp.where(spot < 0, -1, spot + rows)], axis=1))
        weight = table[2 + k : 3 + k]
        factors.append(jnp.concatenate([jnp.ones_like(weight), weight], axis=1))
    x_all = jnp.concatenate([x_ref[...], x_other_ref[...]], axis=0)
    c_all = jnp.concatenate([c_ref[...], c_other_ref[...]], axis=0)
    step = total // 4

    def block(i, carry):
        row = lax.broadcasted_iota(jnp.int32, (step, 2 * count), 0) + i * step
        hits = [row == spots[k] for k in range(2)]
        scale = jnp.sum(
            jnp.where(hits[0], factors[0], 0.0) + jnp.where(hits[1], factors[1], 0.0),
            axis=1,
            keepdims=True,
        )
        pick = jnp.where(hits[0] | hits[1], 1.0, 0.0).astype(bf16)
        made = dot(pick[:, :count], x_all) + dot(pick[:, count:], c_all)
        sent_ref[pl.ds(pl.multiple_of(i * step, step), step), :] = (made * scale).astype(bf16)
        return carry

    lax.fori_loop(0, total // step, block, 0)


def route(core, mine, other, x, x_other, c, c_other, chips, rows):
    vmem = pl.BlockSpec(memory_space=pltpu.VMEM)
    return pl.pallas_call(
        route_kernel,
        in_specs=[pl.BlockSpec(memory_space=pltpu.SMEM)] + [vmem] * 6,
        out_shape=(
            jax.ShapeDtypeStruct((chips * 2 * rows, x.shape[1]), bf16),
            jax.ShapeDtypeStruct((rows - 4, 2 * x.shape[0]), jnp.int32),
        ),
    )(core.reshape(1), mine, other, x, x_other, c, c_other)


GROUP = 4
ROWS = 24


def spread_kernel(own_ref, low_ref, up_ref, far_ref, sent_ref):
    slots, width = own_ref.shape
    cut = width // 2
    part = slots // (sent_ref.shape[0] // ROWS // GROUP)
    out_row = lax.broadcasted_iota(jnp.int32, (2 * part, part), 0)
    slot = lax.broadcasted_iota(jnp.int32, (2 * part, part), 1)
    rows = part // GROUP
    chip = sum((slot >= k * rows).astype(jnp.int32) for k in range(1, GROUP))
    perms = [
        jnp.where(slot + chip * rows + j * rows == out_row, 1.0, 0.0).astype(bf16)
        for j in range(2)
    ]

    def block(i, carry):
        here = pl.ds(pl.multiple_of(i * part, part), part)
        total = own_ref[here, :].astype(f32) + low_ref[here, :].astype(f32)
        total = total + up_ref[here, :].astype(f32) + far_ref[here, :].astype(f32)
        total = total.astype(bf16)
        made = dot(perms[0], total[:, :cut]) + dot(perms[1], total[:, cut:])
        start = pl.multiple_of(i * 2 * part, 2 * part)
        sent_ref[pl.ds(start, 2 * part), :] = made.astype(bf16)
        return carry

    lax.fori_loop(0, slots // part, block, 0)


def spread(own, low, up, far):
    shape = jax.ShapeDtypeStruct((2 * own.shape[0], own.shape[1] // 2), bf16)
    return pl.pallas_call(spread_kernel, out_shape=shape)(own, low, up, far)


def mix_kernel(delta_ref, value_ref, write_ref, read_ref, wide_ref, row_ref, base_ref):
    half = value_ref.shape[1]
    write = write_ref[...]
    read = read_ref[...]
    common = dot(write, read, 1, 1)
    score = None
    turned = None
    for h in range(half // HEAD_DIM):
        lanes = slice(h * HEAD_DIM, (h + 1) * HEAD_DIM)
        mix = jnp.exp(-jnp.abs(wide_ref[:, h * HEAD_DIM : h * HEAD_DIM + 1] - row_ref[h : h + 1, :]))
        delta = delta_ref[:, lanes]
        value = value_ref[:, lanes]
        base_ref[:, lanes] = dot((mix * common).astype(bf16), delta)
        here = dot(delta, value, 1, 1) * mix
        there = dot(value, delta, 1, 1) * mix
        score = here if score is None else score + here
        turned = there if turned is None else turned + there
    base_ref[:, half : half + STATE] = dot(turned.astype(bf16), read)
    base_ref[:, half + STATE :] = dot(score.astype(bf16), write)


def mix_chunk(delta, value, write, read, wide, row):
    shape = jax.ShapeDtypeStruct((value.shape[0], value.shape[1] + 2 * STATE), f32)
    return pl.pallas_call(mix_kernel, out_shape=shape)(delta, value, write, read, wide, row)


def join_kernel(core_ref, mine_ref, got_ref, value_ref, write_ref, read_ref):
    half = value_ref.shape[1] // 2
    lead = core_ref[0] == 0
    mine = mine_ref[...]
    got = got_ref[...].astype(f32)
    value_ref[:, :half] = jnp.where(lead, mine[:, :half], got[:, :half]).astype(bf16)
    value_ref[:, half:] = jnp.where(lead, got[:, :half], mine[:, :half]).astype(bf16)
    sums = (mine[:, half:] + got[:, half:]).astype(bf16)
    write_ref[...] = sums[:, :STATE]
    read_ref[...] = sums[:, STATE:]


def join(core, mine, got):
    rows, width = mine.shape
    vmem = pl.BlockSpec(memory_space=pltpu.VMEM)
    narrow = jax.ShapeDtypeStruct((rows, STATE), bf16)
    return pl.pallas_call(
        join_kernel,
        in_specs=[pl.BlockSpec(memory_space=pltpu.SMEM), vmem, vmem],
        out_shape=(jax.ShapeDtypeStruct((rows, 2 * (width - 2 * STATE)), bf16), narrow, narrow),
    )(core.reshape(1), mine, got)


def scan_kernel(msg_ref, out_ref, work_ref):
    chunks, height, _ = out_ref.shape
    work_ref[...] = msg_ref[...].astype(f32)
    fades = [
        jnp.exp(-(work_ref[k, height : height + 1, :] + work_ref[k, height + 1 : height + 2, :]))
        for k in range(chunks)
    ]
    states = [jnp.zeros((8, 128), f32)] * (height // 8)
    for i in range(chunks):
        for s in range(height // 8):
            k = i if s % 2 == 0 else chunks - 1 - i
            rows = slice(s * 8, s * 8 + 8)
            own = work_ref[k, rows, :]
            work_ref[k, rows, :] = states[s]
            states[s] = states[s] * fades[k] + own
    out_ref[...] = work_ref[:, :height, :].astype(bf16)


def scan_chunks(msg):
    chunks, height, lanes = msg.shape
    return pl.pallas_call(
        scan_kernel,
        out_shape=jax.ShapeDtypeStruct((chunks, height - 8, lanes), bf16),
        scratch_shapes=[pltpu.VMEM(msg.shape, f32)],
    )(msg)


def tail_kernel(
    core_ref,
    back_ref,
    write_ref,
    value_start_ref,
    value_end_ref,
    delta_start_ref,
    delta_end_ref,
    fade_start_ref,
    fade_end_ref,
    base_ref,
    mine_ref,
    send_ref,
    work_ref,
):
    blocks = value_start_ref.shape[1] // 128
    steps = back_ref.shape[0] // blocks
    half = blocks * 128
    write = write_ref[...]
    write_sum = base_ref[:, half : half + STATE]
    read_sum = base_ref[:, half + STATE :]
    for q in range(blocks):
        states = back_ref[q * steps : (q + 1) * steps].astype(f32)
        read_low, read_high, write_low, write_high = (
            states[:, 8 * i : 8 * i + 8, :].reshape(STATE, 128).astype(bf16) for i in range(4)
        )
        lanes = slice(q * 128, (q + 1) * 128)
        work_ref[:, lanes] = (
            base_ref[:, lanes]
            + dot(write, read_low) * fade_start_ref[:, lanes]
            + dot(write, read_high) * fade_end_ref[:, lanes]
        )
        write_sum = write_sum + dot(value_start_ref[:, lanes], read_low, 1, 1)
        write_sum = write_sum + dot(value_end_ref[:, lanes], read_high, 1, 1)
        read_sum = read_sum + dot(delta_start_ref[:, lanes], write_low, 1, 1)
        read_sum = read_sum + dot(delta_end_ref[:, lanes], write_high, 1, 1)
    work_ref[:, half : half + STATE] = write_sum
    work_ref[:, half + STATE :] = read_sum
    tokens = mine_ref.shape[0]
    mine_ref[...] = work_ref[pl.ds(pl.multiple_of(core_ref[0] * tokens, tokens), tokens), :]
    send_ref[...] = work_ref[
        pl.ds(pl.multiple_of((1 - core_ref[0]) * tokens, tokens), tokens), :
    ].astype(bf16)


def tail(core, back, write, value_start, value_end, delta_start, delta_end, fades, base):
    rows, width = base.shape
    vmem = pl.BlockSpec(memory_space=pltpu.VMEM)
    return pl.pallas_call(
        tail_kernel,
        in_specs=[pl.BlockSpec(memory_space=pltpu.SMEM)] + [vmem] * 9,
        out_shape=(
            jax.ShapeDtypeStruct((rows // 2, width), f32),
            jax.ShapeDtypeStruct((rows // 2, width), bf16),
        ),
        scratch_shapes=[pltpu.VMEM((rows, width), f32)],
    )(core.reshape(1), back, write, value_start, value_end, delta_start, delta_end, *fades, base)


def to_message(low, high):
    def cut(a):
        n, w = a.shape
        return a.astype(bf16).reshape(n // 8, 8, w // 128, 128).transpose(2, 0, 1, 3)

    both = jnp.stack([cut(low), cut(high)], axis=2)
    return both.reshape(-1, 16, 128)


def on_device(
    layer_input,
    cotangent,
    routes,
    route_weight,
    gate_weight,
    up_weight,
    down_weight,
    heads_value,
    output_gate,
    mixer_saved,
    proj_weight,
    state_write,
    state_read,
    decay_rate,
):
    core = lax.axis_index(CORE)
    tp = lax.axis_index(TP)
    first = core == 0
    tokens, width = layer_input.shape
    chips = lax.axis_size(CHIPS)
    experts = 2 * chips
    cap = max(2, 3 * tokens * routes.shape[1] // (2 * experts))
    rows = 2 * cap
    n_tp = lax.axis_size(TP)
    heads = decay_rate.shape[1]
    half_heads = heads // 2
    half = heads_value.shape[1] // 2

    def ordered(mine, other, axis=0):
        return jnp.concatenate(
            [jnp.where(first, mine, other), jnp.where(first, other, mine)], axis=axis
        )

    def halves(a):
        left, right = a[:, : a.shape[1] // 2], a[:, a.shape[1] // 2 :]
        return jnp.where(first, left, right), jnp.where(first, right, left)

    small = jnp.concatenate([routes.T.astype(f32), route_weight.T, decay_rate.T], axis=0)
    small_other = swap(small)
    input_other = swap(layer_input)
    cotangent_other = swap(cotangent)
    sent, spot = route(
        core,
        small,
        small_other,
        layer_input,
        input_other,
        cotangent,
        cotangent_other,
        chips,
        rows,
    )
    later_inputs = (gate_weight, up_weight, down_weight, heads_value, output_gate, mixer_saved)
    later_inputs += (proj_weight, state_write, state_read, small, small_other)
    sent, later_inputs = lax.optimization_barrier((sent, later_inputs))
    gate_weight, up_weight, down_weight, heads_value, output_gate, mixer_saved = later_inputs[:6]
    proj_weight, state_write, state_read, small, small_other = later_inputs[6:]

    spot_row = lax.broadcasted_iota(jnp.int32, (chips * 2 * rows, 2 * tokens), 0)
    back = [
        sum(
            jnp.where((spot[k : k + 1] >= 0) & (spot_row == spot[k : k + 1] + j * rows), 1.0, 0.0)
            for k in range(2)
        ).astype(bf16)
        for j in range(2)
    ]

    active_gate, slope_gate = silu_parts(output_gate.astype(f32))
    saved = mixer_saved.astype(f32)
    gated = (saved * active_gate).astype(bf16)
    value_mine, value_send = halves(heads_value)
    side = jnp.concatenate([value_send, state_write, state_read, gated], axis=1)
    side_other = swap(side)
    slots = chips * rows
    slots = chips * rows
    out_row = lax.broadcasted_iota(jnp.int32, (slots, 2 * slots), 0)
    in_row = lax.broadcasted_iota(jnp.int32, (slots, 2 * slots), 1)
    origin = out_row + out_row // rows * rows
    sort_rows = [(origin + j * rows == in_row).astype(bf16) for j in range(2)]
    side_other, small, small_other, back, sort_rows = lax.optimization_barrier(
        (side_other, small, small_other, back, sort_rows)
    )
    value = ordered(value_mine, side_other[:, :half])
    gated_all = jnp.concatenate([gated, side_other[:, half + 2 * STATE :]], axis=0)
    write = ordered(state_write, side_other[:, half : half + STATE])
    read = ordered(state_read, side_other[:, half + STATE : half + 2 * STATE])
    rates = ordered(
        *(jnp.where(first, a[4 : 4 + half_heads], a[4 + half_heads :]) for a in (small, small_other)),
        axis=1,
    )
    cumul_row = jnp.cumsum(rates, axis=1)
    spread_heads = (
        lax.broadcasted_iota(jnp.int32, (half_heads, half), 1) // HEAD_DIM
        == lax.broadcasted_iota(jnp.int32, (half_heads, half), 0)
    ).astype(f32)
    cumul_wide = lax.dot_general(
        cumul_row,
        spread_heads,
        (((0,), (0,)), ((), ())),
        precision=lax.Precision.HIGHEST,
        preferred_element_type=f32,
    )
    total_wide = cumul_wide[-1:]
    fade_end = jnp.exp(cumul_wide - total_wide)
    fade_start = jnp.exp(-cumul_wide)
    value_f = value.astype(f32)
    value_end = (value_f * fade_end).astype(bf16)
    value_start = (value_f * fade_start).astype(bf16)
    write_states = to_message(dot(write, value_end, 0, 0), dot(write, value_start, 0, 0))
    total_high = lax.reduce_precision(total_wide, 8, 7)
    total_rows = jnp.concatenate(
        [total_high, total_wide - total_high, jnp.zeros((6, half), f32)], axis=0
    ).astype(bf16)
    total_rows = jnp.broadcast_to(
        total_rows.reshape(8, half // 128, 1, 128).transpose(1, 2, 0, 3),
        (half // 128, STATE // 8, 8, 128),
    ).reshape(-1, 8, 128)
    quarter = width

    def rolled(a):
        parts = a.reshape(n_tp, quarter, a.shape[1])
        return [
            lax.dynamic_index_in_dim(parts, (tp + i) & (n_tp - 1), 0, keepdims=False)
            for i in range(n_tp)
        ]

    def unrolled(parts):
        stack = jnp.stack(parts)
        return [
            lax.dynamic_index_in_dim(stack, (k + n_tp - tp) & (n_tp - 1), 0, keepdims=False)
            for k in range(n_tp)
        ]

    gate_up = [
        jnp.concatenate(pair, axis=1) for pair in zip(rolled(gate_weight[0]), rolled(up_weight[0]))
    ]
    down = [
        lax.dynamic_slice_in_dim(down_weight[0], ((tp + i) & (n_tp - 1)) * quarter, quarter, 1)
        for i in range(n_tp)
    ]
    proj = rolled(proj_weight)
    hid = gate_weight.shape[2]
    received = exchange(sent.reshape(chips, 2 * rows, width)).reshape(2 * slots, width)
    input_own, cotangent_own = (dot(a, received).astype(bf16) for a in sort_rows)
    input_low = ring(input_own, 1)
    cotangent_up = ring(cotangent_own, -1)
    input_up = ring(input_own, -1)
    cotangent_low = ring(cotangent_own, 1)
    input_far = ring(input_low, 1)
    cotangent_far = ring(cotangent_up, -1)
    input_parts = [input_own, input_up, input_far, input_low]
    cotangent_parts = [cotangent_own, cotangent_up, cotangent_far, cotangent_low]
    order = (0, 1, 3, 2)
    pre = sum(dot(input_parts[i], gate_up[i]) for i in order)
    hidden_grad = sum(dot(cotangent_parts[i], down[i], 1, 1) for i in order)
    pre_gate, pre_up = pre[:, :hid], pre[:, hid:]
    active, slope = silu_parts(pre_gate)
    hidden = (active * pre_up).astype(bf16)
    deltas = jnp.concatenate(
        [(hidden_grad * pre_up * slope).astype(bf16), (hidden_grad * active).astype(bf16)], axis=1
    )
    ready = (write, read, value, gated_all, fade_end, fade_start, value_end, value_start)
    ready += (write_states, total_rows, cumul_wide, cumul_row)
    deltas, ready = lax.optimization_barrier((deltas, ready))
    write, read, value, gated_all, fade_end, fade_start, value_end, value_start = ready[:8]
    write_states, total_rows, cumul_wide, cumul_row = ready[8:]
    partial = [dot(deltas, gate_up[i], 1, 1).astype(bf16) for i in range(n_tp)]
    own, right, far, left = partial
    opposite = ring(far, 2)
    returned = spread(own, ring(right, 1), ring(left, -1), opposite)
    returned, deltas, hidden = lax.optimization_barrier((returned, deltas, hidden))
    cut = width // 2
    arrived = exchange(returned.reshape(chips, 2 * rows, cut))
    arrived = arrived.reshape(2 * slots, cut)

    both_grad = unrolled([dot(input_parts[i], deltas, 0, 0).astype(bf16) for i in range(n_tp)])
    gate_grad = jnp.concatenate([a[:, :hid] for a in both_grad], axis=0)[None]
    up_grad = jnp.concatenate([a[:, hid:] for a in both_grad], axis=0)[None]
    down_grad = jnp.concatenate(
        unrolled([dot(hidden, cotangent_parts[i], 0, 0).astype(bf16) for i in range(n_tp)]), axis=1
    )[None]

    arrived, gate_grad, up_grad, down_grad = lax.optimization_barrier(
        (arrived, gate_grad, up_grad, down_grad)
    )
    summed = jnp.concatenate([dot(back[0], arrived, 0, 0), dot(back[1], arrived, 0, 0)], axis=1)
    summed_other = swap(summed[tokens:].astype(bf16)).astype(f32)
    layer_grad = (cotangent.astype(f32) + summed[:tokens] + summed_other).astype(bf16)
    grads = [layer_grad, ring(layer_grad, -1), ring(layer_grad, 2), ring(layer_grad, 1)]
    out_delta = sum(dot(grads[i], proj[i]) for i in (0, 1, 3, 2)).astype(bf16).astype(f32)
    outgate_grad = (out_delta * saved * slope_gate).astype(bf16)
    mixer_delta = (out_delta * active_gate).astype(bf16)
    delta_mine, delta_send = halves(mixer_delta)
    delta = ordered(delta_mine, swap(delta_send))
    delta_f = delta.astype(f32)
    delta_end = (delta_f * fade_end).astype(bf16)
    delta_start = (delta_f * fade_start).astype(bf16)
    read_states = to_message(dot(read, delta_end, 0, 0), dot(read, delta_start, 0, 0))
    states_got = exchange(jnp.concatenate([read_states, write_states, total_rows], axis=1))

    grad_mine = jnp.concatenate(grads, axis=1)
    grad_all = jnp.concatenate([grad_mine, swap(grad_mine)], axis=0)
    proj_part = dot(grad_all, gated_all, 0, 0).astype(bf16)
    deep, wide = lax.axis_size(SP[0]), lax.axis_size(SP[1])
    block = proj_part.shape[0] // chips // 2
    across = lax.axis_index(SP[1])
    pieces = proj_part.reshape(n_tp, deep // n_tp, wide, 2, block, width)
    pieces = lax.dynamic_index_in_dim(pieces, core, 3, keepdims=False)
    proj_part = jnp.stack(unrolled([pieces[i] for i in range(n_tp)]))
    proj_sum = ring_reduce(
        [
            lax.dynamic_index_in_dim(
                proj_part, (across + i) & (wide - 1), 2, keepdims=False
            ).reshape(deep, block, width)
            for i in range(wide)
        ],
        SP[1],
    )
    scanned = scan_chunks(states_got)
    states_back = exchange(scanned)
    depth = lax.axis_index(SP[0])
    upper = (depth & 1) != 0
    pairs = proj_sum.reshape(deep // 2, 2, block, width)
    away = jnp.where(upper, pairs[:, 0], pairs[:, 1]).astype(bf16)
    got = lax.ppermute(away, SP[0], [(i, i ^ 1) for i in range(deep)])
    proj_sum = jnp.where(upper, pairs[:, 1], pairs[:, 0]) + got.astype(f32)
    level = depth >> 1
    count = deep // 2

    def level_part(i):
        return lax.dynamic_index_in_dim(proj_sum, (level + i) & (count - 1), 0, keepdims=False)

    others = [
        lax.ppermute(
            level_part(k).astype(bf16), SP[0], [(i, (i + 2 * k) % deep) for i in range(deep)]
        )
        for k in range(1, count)
    ]
    proj_grad = level_part(0) + sum(a.astype(f32) for a in others)

    base = mix_chunk(delta, value, write, read, cumul_wide, cumul_row)
    outs_mine, outs_send = tail(
        core,
        states_back,
        write,
        value_start,
        value_end,
        delta_start,
        delta_end,
        (fade_start, fade_end),
        base,
    )
    outs_got = swap(outs_send)
    value_out, write_out, read_out = join(core, outs_mine, outs_got)
    return (
        gate_grad,
        up_grad,
        down_grad,
        proj_grad,
        value_out,
        write_out,
        read_out,
        outgate_grad,
    )


def solution(mesh):
    split = Mesh(mesh.devices.reshape(8, 4, 2, mesh.shape["tp"]), SP + (TP,))
    placed = (
        P(SP, TP),
        P(SP, TP),
        P(SP, None),
        P(SP, None),
        P(SP, None, TP),
        P(SP, None, TP),
        P(SP, TP, None),
        P(SP, TP),
        P(SP, TP),
        P(SP, TP),
        P(None, TP),
        P(SP, TP),
        P(SP, TP),
        P(SP, TP),
    )

    return jax.shard_map(
        on_device,
        mesh=split,
        in_specs=placed,
        out_specs=(
            P(SP, None, TP),
            P(SP, None, TP),
            P(SP, TP, None),
            P(SP, TP),
            P(SP, TP),
            P(SP, TP),
            P(SP, TP),
            P(SP, TP),
        ),
        check_vma=False,
    )
```

```python
import jax
import jax.numpy as jnp
from jax import lax
from jax.experimental import pallas as pl
from jax.experimental.pallas import tpu as pltpu
from jax.sharding import Mesh
from jax.sharding import PartitionSpec as P


HEAD_DIM = 64
STATE = 128
SP = ("sp_0", "sp_1", "sp_2")
CHIPS = ("sp_0", "sp_1")
CORE = "sp_2"
TP = "tp"

f32 = jnp.float32
bf16 = jnp.bfloat16


def dot(a, b, ca=1, cb=0):
    return lax.dot_general(a, b, (((ca,), (cb,)), ((), ())), preferred_element_type=f32)


def swap(x):
    return lax.ppermute(x, CORE, [(0, 1), (1, 0)])


def ring(x, shift, axis=TP):
    n = lax.axis_size(axis)
    return lax.ppermute(x, axis, [(i, (i + shift) % n) for i in range(n)])


def ring_reduce(parts, axis):
    own, right, far, left = parts
    opposite = ring(far, 2, axis)
    low = ring(right, 1, axis)
    up = ring(left, -1, axis)
    return own.astype(f32) + low.astype(f32) + up.astype(f32) + opposite.astype(f32)


def exchange(x):
    return lax.all_to_all(x, CHIPS, split_axis=0, concat_axis=0, tiled=True)


def silu_parts(value):
    sigma = jax.nn.sigmoid(value)
    return (value * sigma, sigma * (1.0 + value * (1.0 - sigma)))


def route_kernel(
    core_ref, mine_ref, other_ref, x_ref, x_other_ref, c_ref, c_other_ref, sent_ref, spot_ref
):
    tokens = x_ref.shape[0]
    count = 2 * tokens
    total = sent_ref.shape[0]
    rows = spot_ref.shape[0] + 4
    cap = rows // 2
    experts = total // rows
    core = core_ref[0]
    table = jnp.concatenate([mine_ref[...], other_ref[...]], axis=1)
    ids = table[0:2].astype(jnp.int32)
    source = (lax.broadcasted_iota(jnp.int32, (1, count), 1) >= tokens).astype(jnp.int32)
    expert_col = lax.broadcasted_iota(jnp.int32, (experts, count), 0)
    named = [expert_col == ids[k : k + 1] for k in range(2)]
    named_any = jnp.where(named[0] | named[1], 1.0, 0.0).astype(bf16)
    earlier = lax.broadcasted_iota(jnp.int32, (count, count), 0)
    later = lax.broadcasted_iota(jnp.int32, (count, count), 1)
    ahead = jnp.where((earlier < later) & ((earlier >= tokens) | (later < tokens)), 1.0, 0.0)
    before = dot(named_any, ahead.astype(bf16))
    spots = []
    factors = []
    for k in range(2):
        rank = jnp.sum(jnp.where(named[k], before, 0.0), axis=0, keepdims=True).astype(jnp.int32)
        expert = ids[k : k + 1]
        spot = jnp.where(
            (expert & 1) == core, (expert >> 1) * (2 * rows) + source * cap + rank, -1
        )
        spot_ref[k : k + 1, :] = spot
        spots.append(jnp.concatenate([spot, jnp.where(spot < 0, -1, spot + rows)], axis=1))
        weight = table[2 + k : 3 + k]
        factors.append(jnp.concatenate([jnp.ones_like(weight), weight], axis=1))
    x_all = jnp.concatenate([x_ref[...], x_other_ref[...]], axis=0)
    c_all = jnp.concatenate([c_ref[...], c_other_ref[...]], axis=0)
    step = total // 4

    def block(i, carry):
        row = lax.broadcasted_iota(jnp.int32, (step, 2 * count), 0) + i * step
        hits = [row == spots[k] for k in range(2)]
        scale = jnp.sum(
            jnp.where(hits[0], factors[0], 0.0) + jnp.where(hits[1], factors[1], 0.0),
            axis=1,
            keepdims=True,
        )
        pick = jnp.where(hits[0] | hits[1], 1.0, 0.0).astype(bf16)
        made = dot(pick[:, :count], x_all) + dot(pick[:, count:], c_all)
        sent_ref[pl.ds(pl.multiple_of(i * step, step), step), :] = (made * scale).astype(bf16)
        return carry

    lax.fori_loop(0, total // step, block, 0)


def route(core, mine, other, x, x_other, c, c_other, chips, rows):
    vmem = pl.BlockSpec(memory_space=pltpu.VMEM)
    return pl.pallas_call(
        route_kernel,
        in_specs=[pl.BlockSpec(memory_space=pltpu.SMEM)] + [vmem] * 6,
        out_shape=(
            jax.ShapeDtypeStruct((chips * 2 * rows, x.shape[1]), bf16),
            jax.ShapeDtypeStruct((rows - 4, 2 * x.shape[0]), jnp.int32),
        ),
    )(core.reshape(1), mine, other, x, x_other, c, c_other)


GROUP = 4
ROWS = 24


def spread_kernel(own_ref, low_ref, up_ref, far_ref, sent_ref):
    slots, width = own_ref.shape
    cut = width // 2
    part = slots // (sent_ref.shape[0] // ROWS // GROUP)
    out_row = lax.broadcasted_iota(jnp.int32, (2 * part, part), 0)
    slot = lax.broadcasted_iota(jnp.int32, (2 * part, part), 1)
    rows = part // GROUP
    chip = sum((slot >= k * rows).astype(jnp.int32) for k in range(1, GROUP))
    perms = [
        jnp.where(slot + chip * rows + j * rows == out_row, 1.0, 0.0).astype(bf16)
        for j in range(2)
    ]

    def block(i, carry):
        here = pl.ds(pl.multiple_of(i * part, part), part)
        total = own_ref[here, :].astype(f32) + low_ref[here, :].astype(f32)
        total = total + up_ref[here, :].astype(f32) + far_ref[here, :].astype(f32)
        total = total.astype(bf16)
        made = dot(perms[0], total[:, :cut]) + dot(perms[1], total[:, cut:])
        start = pl.multiple_of(i * 2 * part, 2 * part)
        sent_ref[pl.ds(start, 2 * part), :] = made.astype(bf16)
        return carry

    lax.fori_loop(0, slots // part, block, 0)


def spread(own, low, up, far):
    shape = jax.ShapeDtypeStruct((2 * own.shape[0], own.shape[1] // 2), bf16)
    return pl.pallas_call(spread_kernel, out_shape=shape)(own, low, up, far)


def mix_kernel(delta_ref, value_ref, write_ref, read_ref, wide_ref, row_ref, base_ref):
    half = value_ref.shape[1]
    write = write_ref[...]
    read = read_ref[...]
    common = dot(write, read, 1, 1)
    score = None
    turned = None
    for h in range(half // HEAD_DIM):
        lanes = slice(h * HEAD_DIM, (h + 1) * HEAD_DIM)
        mix = jnp.exp(-jnp.abs(wide_ref[:, h * HEAD_DIM : h * HEAD_DIM + 1] - row_ref[h : h + 1, :]))
        delta = delta_ref[:, lanes]
        value = value_ref[:, lanes]
        base_ref[:, lanes] = dot((mix * common).astype(bf16), delta)
        here = dot(delta, value, 1, 1) * mix
        there = dot(value, delta, 1, 1) * mix
        score = here if score is None else score + here
        turned = there if turned is None else turned + there
    base_ref[:, half : half + STATE] = dot(turned.astype(bf16), read)
    base_ref[:, half + STATE :] = dot(score.astype(bf16), write)


def mix_chunk(delta, value, write, read, wide, row):
    shape = jax.ShapeDtypeStruct((value.shape[0], value.shape[1] + 2 * STATE), f32)
    return pl.pallas_call(mix_kernel, out_shape=shape)(delta, value, write, read, wide, row)


def join_kernel(core_ref, mine_ref, got_ref, value_ref, write_ref, read_ref):
    half = value_ref.shape[1] // 2
    lead = core_ref[0] == 0
    mine = mine_ref[...]
    got = got_ref[...].astype(f32)
    value_ref[:, :half] = jnp.where(lead, mine[:, :half], got[:, :half]).astype(bf16)
    value_ref[:, half:] = jnp.where(lead, got[:, :half], mine[:, :half]).astype(bf16)
    sums = (mine[:, half:] + got[:, half:]).astype(bf16)
    write_ref[...] = sums[:, :STATE]
    read_ref[...] = sums[:, STATE:]


def join(core, mine, got):
    rows, width = mine.shape
    vmem = pl.BlockSpec(memory_space=pltpu.VMEM)
    narrow = jax.ShapeDtypeStruct((rows, STATE), bf16)
    return pl.pallas_call(
        join_kernel,
        in_specs=[pl.BlockSpec(memory_space=pltpu.SMEM), vmem, vmem],
        out_shape=(jax.ShapeDtypeStruct((rows, 2 * (width - 2 * STATE)), bf16), narrow, narrow),
    )(core.reshape(1), mine, got)


def scan_kernel(msg_ref, out_ref, work_ref):
    chunks, height, _ = out_ref.shape
    work_ref[...] = msg_ref[...].astype(f32)
    fades = [
        jnp.exp(-(work_ref[k, height : height + 1, :] + work_ref[k, height + 1 : height + 2, :]))
        for k in range(chunks)
    ]
    states = [jnp.zeros((8, 128), f32)] * (height // 8)
    for i in range(chunks):
        for s in range(height // 8):
            k = i if s % 2 == 0 else chunks - 1 - i
            rows = slice(s * 8, s * 8 + 8)
            own = work_ref[k, rows, :]
            work_ref[k, rows, :] = states[s]
            states[s] = states[s] * fades[k] + own
    out_ref[...] = work_ref[:, :height, :].astype(bf16)


def scan_chunks(msg):
    chunks, height, lanes = msg.shape
    return pl.pallas_call(
        scan_kernel,
        out_shape=jax.ShapeDtypeStruct((chunks, height - 8, lanes), bf16),
        scratch_shapes=[pltpu.VMEM(msg.shape, f32)],
    )(msg)


def tail_kernel(
    core_ref,
    back_ref,
    write_ref,
    value_start_ref,
    value_end_ref,
    delta_start_ref,
    delta_end_ref,
    fade_start_ref,
    fade_end_ref,
    base_ref,
    mine_ref,
    send_ref,
    work_ref,
):
    blocks = value_start_ref.shape[1] // 128
    steps = back_ref.shape[0] // blocks
    half = blocks * 128
    write = write_ref[...]
    write_sum = base_ref[:, half : half + STATE]
    read_sum = base_ref[:, half + STATE :]
    for q in range(blocks):
        states = back_ref[q * steps : (q + 1) * steps].astype(f32)
        read_low, read_high, write_low, write_high = (
            states[:, 8 * i : 8 * i + 8, :].reshape(STATE, 128).astype(bf16) for i in range(4)
        )
        lanes = slice(q * 128, (q + 1) * 128)
        work_ref[:, lanes] = (
            base_ref[:, lanes]
            + dot(write, read_low) * fade_start_ref[:, lanes]
            + dot(write, read_high) * fade_end_ref[:, lanes]
        )
        write_sum = write_sum + dot(value_start_ref[:, lanes], read_low, 1, 1)
        write_sum = write_sum + dot(value_end_ref[:, lanes], read_high, 1, 1)
        read_sum = read_sum + dot(delta_start_ref[:, lanes], write_low, 1, 1)
        read_sum = read_sum + dot(delta_end_ref[:, lanes], write_high, 1, 1)
    work_ref[:, half : half + STATE] = write_sum
    work_ref[:, half + STATE :] = read_sum
    tokens = mine_ref.shape[0]
    mine_ref[...] = work_ref[pl.ds(pl.multiple_of(core_ref[0] * tokens, tokens), tokens), :]
    send_ref[...] = work_ref[
        pl.ds(pl.multiple_of((1 - core_ref[0]) * tokens, tokens), tokens), :
    ].astype(bf16)


def tail(core, back, write, value_start, value_end, delta_start, delta_end, fades, base):
    rows, width = base.shape
    vmem = pl.BlockSpec(memory_space=pltpu.VMEM)
    return pl.pallas_call(
        tail_kernel,
        in_specs=[pl.BlockSpec(memory_space=pltpu.SMEM)] + [vmem] * 9,
        out_shape=(
            jax.ShapeDtypeStruct((rows // 2, width), f32),
            jax.ShapeDtypeStruct((rows // 2, width), bf16),
        ),
        scratch_shapes=[pltpu.VMEM((rows, width), f32)],
    )(core.reshape(1), back, write, value_start, value_end, delta_start, delta_end, *fades, base)


def to_message(low, high):
    def cut(a):
        n, w = a.shape
        return a.astype(bf16).reshape(n // 8, 8, w // 128, 128).transpose(2, 0, 1, 3)

    both = jnp.stack([cut(low), cut(high)], axis=2)
    return both.reshape(-1, 16, 128)


def on_device(
    layer_input,
    cotangent,
    routes,
    route_weight,
    gate_weight,
    up_weight,
    down_weight,
    heads_value,
    output_gate,
    mixer_saved,
    proj_weight,
    state_write,
    state_read,
    decay_rate,
):
    core = lax.axis_index(CORE)
    tp = lax.axis_index(TP)
    first = core == 0
    tokens, width = layer_input.shape
    chips = lax.axis_size(CHIPS)
    experts = 2 * chips
    cap = max(2, 3 * tokens * routes.shape[1] // (2 * experts))
    rows = 2 * cap
    n_tp = lax.axis_size(TP)
    heads = decay_rate.shape[1]
    half_heads = heads // 2
    half = heads_value.shape[1] // 2

    def ordered(mine, other, axis=0):
        return jnp.concatenate(
            [jnp.where(first, mine, other), jnp.where(first, other, mine)], axis=axis
        )

    def halves(a):
        left, right = a[:, : a.shape[1] // 2], a[:, a.shape[1] // 2 :]
        return jnp.where(first, left, right), jnp.where(first, right, left)

    small = jnp.concatenate([routes.T.astype(f32), route_weight.T, decay_rate.T], axis=0)
    small_other = swap(small)
    input_other = swap(layer_input)
    cotangent_other = swap(cotangent)
    sent, spot = route(
        core,
        small,
        small_other,
        layer_input,
        input_other,
        cotangent,
        cotangent_other,
        chips,
        rows,
    )
    later_inputs = (gate_weight, up_weight, down_weight, heads_value, output_gate, mixer_saved)
    later_inputs += (proj_weight, state_write, state_read, small, small_other)
    sent, later_inputs = lax.optimization_barrier((sent, later_inputs))
    gate_weight, up_weight, down_weight, heads_value, output_gate, mixer_saved = later_inputs[:6]
    proj_weight, state_write, state_read, small, small_other = later_inputs[6:]

    spot_row = lax.broadcasted_iota(jnp.int32, (chips * 2 * rows, 2 * tokens), 0)
    back = [
        sum(
            jnp.where((spot[k : k + 1] >= 0) & (spot_row == spot[k : k + 1] + j * rows), 1.0, 0.0)
            for k in range(2)
        ).astype(bf16)
        for j in range(2)
    ]

    active_gate, slope_gate = silu_parts(output_gate.astype(f32))
    saved = mixer_saved.astype(f32)
    gated = (saved * active_gate).astype(bf16)
    value_mine, value_send = halves(heads_value)
    side = jnp.concatenate([value_send, state_write, state_read, gated], axis=1)
    side_other = swap(side)
    slots = chips * rows
    slots = chips * rows
    out_row = lax.broadcasted_iota(jnp.int32, (slots, 2 * slots), 0)
    in_row = lax.broadcasted_iota(jnp.int32, (slots, 2 * slots), 1)
    origin = out_row + out_row // rows * rows
    sort_rows = [(origin + j * rows == in_row).astype(bf16) for j in range(2)]
    side_other, small, small_other, back, sort_rows = lax.optimization_barrier(
        (side_other, small, small_other, back, sort_rows)
    )
    value = ordered(value_mine, side_other[:, :half])
    gated_all = jnp.concatenate([gated, side_other[:, half + 2 * STATE :]], axis=0)
    write = ordered(state_write, side_other[:, half : half + STATE])
    read = ordered(state_read, side_other[:, half + STATE : half + 2 * STATE])
    rates = ordered(
        *(jnp.where(first, a[4 : 4 + half_heads], a[4 + half_heads :]) for a in (small, small_other)),
        axis=1,
    )
    cumul_row = jnp.cumsum(rates, axis=1)
    head_of = lax.broadcasted_iota(jnp.int32, (half_heads, half), 0) * HEAD_DIM
    lane = lax.broadcasted_iota(jnp.int32, (half_heads, half), 1)
    spread_heads = ((lane >= head_of) & (lane < head_of + HEAD_DIM)).astype(f32)
    cumul_wide = lax.dot_general(
        cumul_row,
        spread_heads,
        (((0,), (0,)), ((), ())),
        precision=lax.Precision.HIGHEST,
        preferred_element_type=f32,
    )
    total_wide = cumul_wide[-1:]
    fade_end = jnp.exp(cumul_wide - total_wide)
    fade_start = jnp.exp(-cumul_wide)
    value_f = value.astype(f32)
    value_end = (value_f * fade_end).astype(bf16)
    value_start = (value_f * fade_start).astype(bf16)
    write_states = to_message(dot(write, value_end, 0, 0), dot(write, value_start, 0, 0))
    total_high = lax.reduce_precision(total_wide, 8, 7)
    row = lax.broadcasted_iota(jnp.int32, (8, half), 0)
    total_low = total_wide - total_high
    total_rows = jnp.where(row == 0, total_high, jnp.where(row == 1, total_low, 0.0)).astype(bf16)
    total_rows = total_rows.reshape(8, half // 128, 1, 128).transpose(1, 2, 0, 3)
    total_rows = jnp.broadcast_to(total_rows, (half // 128, STATE // 8, 8, 128))
    total_rows = total_rows.reshape(-1, 8, 128)
    quarter = width

    def rolled(a):
        parts = a.reshape(n_tp, quarter, a.shape[1])
        return [
            lax.dynamic_index_in_dim(parts, (tp + i) & (n_tp - 1), 0, keepdims=False)
            for i in range(n_tp)
        ]

    def unrolled(parts):
        stack = jnp.stack(parts)
        return [
            lax.dynamic_index_in_dim(stack, (k + n_tp - tp) & (n_tp - 1), 0, keepdims=False)
            for k in range(n_tp)
        ]

    gate_up = [
        jnp.concatenate(pair, axis=1) for pair in zip(rolled(gate_weight[0]), rolled(up_weight[0]))
    ]
    down = [
        lax.dynamic_slice_in_dim(down_weight[0], ((tp + i) & (n_tp - 1)) * quarter, quarter, 1)
        for i in range(n_tp)
    ]
    proj = rolled(proj_weight)
    hid = gate_weight.shape[2]
    received = exchange(sent.reshape(chips, 2 * rows, width)).reshape(2 * slots, width)
    ready = (write, read, value, gated_all, fade_end, fade_start, value_end, value_start)
    ready += (write_states, total_rows, cumul_wide, cumul_row)
    received, ready = lax.optimization_barrier((received, ready))
    write, read, value, gated_all, fade_end, fade_start, value_end, value_start = ready[:8]
    write_states, total_rows, cumul_wide, cumul_row = ready[8:]
    input_own, cotangent_own = (dot(a, received).astype(bf16) for a in sort_rows)
    input_low = ring(input_own, 1)
    cotangent_up = ring(cotangent_own, -1)
    input_up = ring(input_own, -1)
    cotangent_low = ring(cotangent_own, 1)
    input_far = ring(input_low, 1)
    cotangent_far = ring(cotangent_up, -1)
    input_parts = [input_own, input_up, input_far, input_low]
    cotangent_parts = [cotangent_own, cotangent_up, cotangent_far, cotangent_low]
    order = (0, 1, 3, 2)
    pre = sum(dot(input_parts[i], gate_up[i]) for i in order)
    hidden_grad = sum(dot(cotangent_parts[i], down[i], 1, 1) for i in order)
    pre_gate, pre_up = pre[:, :hid], pre[:, hid:]
    active, slope = silu_parts(pre_gate)
    hidden = (active * pre_up).astype(bf16)
    deltas = jnp.concatenate(
        [(hidden_grad * pre_up * slope).astype(bf16), (hidden_grad * active).astype(bf16)], axis=1
    )
    opposite = ring(dot(deltas, gate_up[2], 1, 1).astype(bf16), 2)
    right, left, own = (dot(deltas, gate_up[i], 1, 1).astype(bf16) for i in (1, 3, 0))
    returned = spread(own, ring(right, 1), ring(left, -1), opposite)
    returned, deltas, hidden = lax.optimization_barrier((returned, deltas, hidden))
    cut = width // 2
    arrived = exchange(returned.reshape(chips, 2 * rows, cut))
    arrived = arrived.reshape(2 * slots, cut)

    both_grad = unrolled([dot(input_parts[i], deltas, 0, 0).astype(bf16) for i in range(n_tp)])
    gate_grad = jnp.concatenate([a[:, :hid] for a in both_grad], axis=0)[None]
    up_grad = jnp.concatenate([a[:, hid:] for a in both_grad], axis=0)[None]
    down_grad = jnp.concatenate(
        unrolled([dot(hidden, cotangent_parts[i], 0, 0).astype(bf16) for i in range(n_tp)]), axis=1
    )[None]

    arrived, gate_grad, up_grad, down_grad = lax.optimization_barrier(
        (arrived, gate_grad, up_grad, down_grad)
    )
    summed = jnp.concatenate([dot(back[0], arrived, 0, 0), dot(back[1], arrived, 0, 0)], axis=1)
    summed_other = swap(summed[tokens:].astype(bf16)).astype(f32)
    layer_grad = (cotangent.astype(f32) + summed[:tokens] + summed_other).astype(bf16)
    grads = [layer_grad, ring(layer_grad, -1), ring(layer_grad, 2), ring(layer_grad, 1)]
    out_delta = sum(dot(grads[i], proj[i]) for i in (0, 1, 3, 2)).astype(bf16).astype(f32)
    outgate_grad = (out_delta * saved * slope_gate).astype(bf16)
    mixer_delta = (out_delta * active_gate).astype(bf16)
    delta_mine, delta_send = halves(mixer_delta)
    delta = ordered(delta_mine, swap(delta_send))
    delta_f = delta.astype(f32)
    delta_end = (delta_f * fade_end).astype(bf16)
    delta_start = (delta_f * fade_start).astype(bf16)
    read_states = to_message(dot(read, delta_end, 0, 0), dot(read, delta_start, 0, 0))
    states_got = exchange(jnp.concatenate([read_states, write_states, total_rows], axis=1))

    grad_mine = jnp.concatenate(grads, axis=1)
    grad_all = jnp.concatenate([grad_mine, swap(grad_mine)], axis=0)
    proj_part = dot(grad_all, gated_all, 0, 0).astype(bf16)
    deep, wide = lax.axis_size(SP[0]), lax.axis_size(SP[1])
    block = proj_part.shape[0] // chips // 2
    across = lax.axis_index(SP[1])
    pieces = proj_part.reshape(n_tp, deep // n_tp, wide, 2, block, width)
    pieces = lax.dynamic_index_in_dim(pieces, core, 3, keepdims=False)
    proj_part = jnp.stack(unrolled([pieces[i] for i in range(n_tp)]))
    proj_sum = ring_reduce(
        [
            lax.dynamic_index_in_dim(
                proj_part, (across + i) & (wide - 1), 2, keepdims=False
            ).reshape(deep, block, width)
            for i in range(wide)
        ],
        SP[1],
    )
    scanned = scan_chunks(states_got)
    states_back = exchange(scanned)
    depth = lax.axis_index(SP[0])
    upper = (depth & 1) != 0
    pairs = proj_sum.reshape(deep // 2, 2, block, width)
    away = jnp.where(upper, pairs[:, 0], pairs[:, 1]).astype(bf16)
    got = lax.ppermute(away, SP[0], [(i, i ^ 1) for i in range(deep)])
    proj_sum = jnp.where(upper, pairs[:, 1], pairs[:, 0]) + got.astype(f32)
    level = depth >> 1
    count = deep // 2

    def level_part(i):
        return lax.dynamic_index_in_dim(proj_sum, (level + i) & (count - 1), 0, keepdims=False)

    others = [
        lax.ppermute(
            level_part(k).astype(bf16), SP[0], [(i, (i + 2 * k) % deep) for i in range(deep)]
        )
        for k in range(1, count)
    ]
    proj_grad = level_part(0) + sum(a.astype(f32) for a in others)

    base = mix_chunk(delta, value, write, read, cumul_wide, cumul_row)
    outs_mine, outs_send = tail(
        core,
        states_back,
        write,
        value_start,
        value_end,
        delta_start,
        delta_end,
        (fade_start, fade_end),
        base,
    )
    outs_got = swap(outs_send)
    value_out, write_out, read_out = join(core, outs_mine, outs_got)
    return (
        gate_grad,
        up_grad,
        down_grad,
        proj_grad,
        value_out,
        write_out,
        read_out,
        outgate_grad,
    )


def solution(mesh):
    split = Mesh(mesh.devices.reshape(8, 4, 2, mesh.shape["tp"]), SP + (TP,))
    placed = (
        P(SP, TP),
        P(SP, TP),
        P(SP, None),
        P(SP, None),
        P(SP, None, TP),
        P(SP, None, TP),
        P(SP, TP, None),
        P(SP, TP),
        P(SP, TP),
        P(SP, TP),
        P(None, TP),
        P(SP, TP),
        P(SP, TP),
        P(SP, TP),
    )

    return jax.shard_map(
        on_device,
        mesh=split,
        in_specs=placed,
        out_specs=(
            P(SP, None, TP),
            P(SP, None, TP),
            P(SP, TP, None),
            P(SP, TP),
            P(SP, TP),
            P(SP, TP),
            P(SP, TP),
            P(SP, TP),
        ),
        check_vma=False,
    )
```

```python
import jax
import jax.numpy as jnp
from jax import lax
from jax.experimental import pallas as pl
from jax.experimental.pallas import tpu as pltpu
from jax.sharding import Mesh
from jax.sharding import PartitionSpec as P


HEAD_DIM = 64
STATE = 128
SP = ("sp_0", "sp_1", "sp_2")
CHIPS = ("sp_0", "sp_1")
CORE = "sp_2"
TP = "tp"

f32 = jnp.float32
bf16 = jnp.bfloat16


def dot(a, b, ca=1, cb=0):
    return lax.dot_general(a, b, (((ca,), (cb,)), ((), ())), preferred_element_type=f32)


def swap(x):
    return lax.ppermute(x, CORE, [(0, 1), (1, 0)])


def ring(x, shift, axis=TP):
    n = lax.axis_size(axis)
    return lax.ppermute(x, axis, [(i, (i + shift) % n) for i in range(n)])


def ring_reduce(parts, axis):
    own, right, far, left = parts
    opposite = ring(far, 2, axis)
    low = ring(right, 1, axis)
    up = ring(left, -1, axis)
    return own.astype(f32) + low.astype(f32) + up.astype(f32) + opposite.astype(f32)


def exchange(x):
    return lax.all_to_all(x, CHIPS, split_axis=0, concat_axis=0, tiled=True)


def silu_parts(value):
    sigma = jax.nn.sigmoid(value)
    return (value * sigma, sigma * (1.0 + value * (1.0 - sigma)))


def route_kernel(
    core_ref, mine_ref, other_ref, x_ref, x_other_ref, c_ref, c_other_ref, sent_ref, spot_ref
):
    tokens = x_ref.shape[0]
    count = 2 * tokens
    total = sent_ref.shape[0]
    rows = spot_ref.shape[0] + 4
    cap = rows // 2
    experts = total // rows
    core = core_ref[0]
    table = jnp.concatenate([mine_ref[...], other_ref[...]], axis=1)
    ids = table[0:2].astype(jnp.int32)
    source = (lax.broadcasted_iota(jnp.int32, (1, count), 1) >= tokens).astype(jnp.int32)
    expert_col = lax.broadcasted_iota(jnp.int32, (experts, count), 0)
    named = [expert_col == ids[k : k + 1] for k in range(2)]
    named_any = jnp.where(named[0] | named[1], 1.0, 0.0).astype(bf16)
    earlier = lax.broadcasted_iota(jnp.int32, (count, count), 0)
    later = lax.broadcasted_iota(jnp.int32, (count, count), 1)
    ahead = jnp.where((earlier < later) & ((earlier >= tokens) | (later < tokens)), 1.0, 0.0)
    before = dot(named_any, ahead.astype(bf16))
    spots = []
    factors = []
    for k in range(2):
        rank = jnp.sum(jnp.where(named[k], before, 0.0), axis=0, keepdims=True).astype(jnp.int32)
        expert = ids[k : k + 1]
        spot = jnp.where(
            (expert & 1) == core, (expert >> 1) * (2 * rows) + source * cap + rank, -1
        )
        spot_ref[k : k + 1, :] = spot
        spots.append(jnp.concatenate([spot, jnp.where(spot < 0, -1, spot + rows)], axis=1))
        weight = table[2 + k : 3 + k]
        factors.append(jnp.concatenate([jnp.ones_like(weight), weight], axis=1))
    x_all = jnp.concatenate([x_ref[...], x_other_ref[...]], axis=0)
    c_all = jnp.concatenate([c_ref[...], c_other_ref[...]], axis=0)
    step = total // 4

    def block(i, carry):
        row = lax.broadcasted_iota(jnp.int32, (step, 2 * count), 0) + i * step
        hits = [row == spots[k] for k in range(2)]
        scale = jnp.sum(
            jnp.where(hits[0], factors[0], 0.0) + jnp.where(hits[1], factors[1], 0.0),
            axis=1,
            keepdims=True,
        )
        pick = jnp.where(hits[0] | hits[1], 1.0, 0.0).astype(bf16)
        made = dot(pick[:, :count], x_all) + dot(pick[:, count:], c_all)
        sent_ref[pl.ds(pl.multiple_of(i * step, step), step), :] = (made * scale).astype(bf16)
        return carry

    lax.fori_loop(0, total // step, block, 0)


def route(core, mine, other, x, x_other, c, c_other, chips, rows):
    vmem = pl.BlockSpec(memory_space=pltpu.VMEM)
    return pl.pallas_call(
        route_kernel,
        in_specs=[pl.BlockSpec(memory_space=pltpu.SMEM)] + [vmem] * 6,
        out_shape=(
            jax.ShapeDtypeStruct((chips * 2 * rows, x.shape[1]), bf16),
            jax.ShapeDtypeStruct((rows - 4, 2 * x.shape[0]), jnp.int32),
        ),
    )(core.reshape(1), mine, other, x, x_other, c, c_other)


GROUP = 4
ROWS = 24


def spread_kernel(own_ref, low_ref, up_ref, far_ref, sent_ref):
    slots, width = own_ref.shape
    cut = width // 2
    part = slots // (sent_ref.shape[0] // ROWS // GROUP)
    out_row = lax.broadcasted_iota(jnp.int32, (2 * part, part), 0)
    slot = lax.broadcasted_iota(jnp.int32, (2 * part, part), 1)
    rows = part // GROUP
    chip = sum((slot >= k * rows).astype(jnp.int32) for k in range(1, GROUP))
    perms = [
        jnp.where(slot + chip * rows + j * rows == out_row, 1.0, 0.0).astype(bf16)
        for j in range(2)
    ]

    def block(i, carry):
        here = pl.ds(pl.multiple_of(i * part, part), part)
        total = own_ref[here, :].astype(f32) + low_ref[here, :].astype(f32)
        total = total + up_ref[here, :].astype(f32) + far_ref[here, :].astype(f32)
        total = total.astype(bf16)
        made = dot(perms[0], total[:, :cut]) + dot(perms[1], total[:, cut:])
        start = pl.multiple_of(i * 2 * part, 2 * part)
        sent_ref[pl.ds(start, 2 * part), :] = made.astype(bf16)
        return carry

    lax.fori_loop(0, slots // part, block, 0)


def spread(own, low, up, far):
    shape = jax.ShapeDtypeStruct((2 * own.shape[0], own.shape[1] // 2), bf16)
    return pl.pallas_call(spread_kernel, out_shape=shape)(own, low, up, far)


def mix_kernel(delta_ref, value_ref, write_ref, read_ref, wide_ref, row_ref, base_ref):
    half = value_ref.shape[1]
    write = write_ref[...]
    read = read_ref[...]
    common = dot(write, read, 1, 1)
    score = None
    turned = None
    for h in range(half // HEAD_DIM):
        lanes = slice(h * HEAD_DIM, (h + 1) * HEAD_DIM)
        mix = jnp.exp(-jnp.abs(wide_ref[:, h * HEAD_DIM : h * HEAD_DIM + 1] - row_ref[h : h + 1, :]))
        delta = delta_ref[:, lanes]
        value = value_ref[:, lanes]
        base_ref[:, lanes] = dot((mix * common).astype(bf16), delta)
        here = dot(delta, value, 1, 1) * mix
        there = dot(value, delta, 1, 1) * mix
        score = here if score is None else score + here
        turned = there if turned is None else turned + there
    base_ref[:, half : half + STATE] = dot(turned.astype(bf16), read)
    base_ref[:, half + STATE :] = dot(score.astype(bf16), write)


def mix_chunk(delta, value, write, read, wide, row):
    shape = jax.ShapeDtypeStruct((value.shape[0], value.shape[1] + 2 * STATE), f32)
    return pl.pallas_call(mix_kernel, out_shape=shape)(delta, value, write, read, wide, row)


def join_kernel(core_ref, mine_ref, got_ref, value_ref, write_ref, read_ref):
    half = value_ref.shape[1] // 2
    lead = core_ref[0] == 0
    mine = mine_ref[...]
    got = got_ref[...].astype(f32)
    value_ref[:, :half] = jnp.where(lead, mine[:, :half], got[:, :half]).astype(bf16)
    value_ref[:, half:] = jnp.where(lead, got[:, :half], mine[:, :half]).astype(bf16)
    sums = (mine[:, half:] + got[:, half:]).astype(bf16)
    write_ref[...] = sums[:, :STATE]
    read_ref[...] = sums[:, STATE:]


def join(core, mine, got):
    rows, width = mine.shape
    vmem = pl.BlockSpec(memory_space=pltpu.VMEM)
    narrow = jax.ShapeDtypeStruct((rows, STATE), bf16)
    return pl.pallas_call(
        join_kernel,
        in_specs=[pl.BlockSpec(memory_space=pltpu.SMEM), vmem, vmem],
        out_shape=(jax.ShapeDtypeStruct((rows, 2 * (width - 2 * STATE)), bf16), narrow, narrow),
    )(core.reshape(1), mine, got)


def scan_kernel(msg_ref, out_ref, work_ref):
    chunks, height, _ = out_ref.shape
    work_ref[...] = msg_ref[...].astype(f32)
    fades = [
        jnp.exp(-(work_ref[k, height : height + 1, :] + work_ref[k, height + 1 : height + 2, :]))
        for k in range(chunks)
    ]
    states = [jnp.zeros((8, 128), f32)] * (height // 8)
    for i in range(chunks):
        for s in range(height // 8):
            k = i if s % 2 == 0 else chunks - 1 - i
            rows = slice(s * 8, s * 8 + 8)
            own = work_ref[k, rows, :]
            work_ref[k, rows, :] = states[s]
            states[s] = states[s] * fades[k] + own
    out_ref[...] = work_ref[:, :height, :].astype(bf16)


def scan_chunks(msg):
    chunks, height, lanes = msg.shape
    return pl.pallas_call(
        scan_kernel,
        out_shape=jax.ShapeDtypeStruct((chunks, height - 8, lanes), bf16),
        scratch_shapes=[pltpu.VMEM(msg.shape, f32)],
    )(msg)


def tail_kernel(
    core_ref,
    back_ref,
    write_ref,
    value_start_ref,
    value_end_ref,
    delta_start_ref,
    delta_end_ref,
    fade_start_ref,
    fade_end_ref,
    base_ref,
    mine_ref,
    send_ref,
    work_ref,
):
    blocks = value_start_ref.shape[1] // 128
    steps = back_ref.shape[0] // blocks
    half = blocks * 128
    write = write_ref[...]
    write_sum = base_ref[:, half : half + STATE]
    read_sum = base_ref[:, half + STATE :]
    for q in range(blocks):
        states = back_ref[q * steps : (q + 1) * steps].astype(f32)
        read_low, read_high, write_low, write_high = (
            states[:, 8 * i : 8 * i + 8, :].reshape(STATE, 128).astype(bf16) for i in range(4)
        )
        lanes = slice(q * 128, (q + 1) * 128)
        work_ref[:, lanes] = (
            base_ref[:, lanes]
            + dot(write, read_low) * fade_start_ref[:, lanes]
            + dot(write, read_high) * fade_end_ref[:, lanes]
        )
        write_sum = write_sum + dot(value_start_ref[:, lanes], read_low, 1, 1)
        write_sum = write_sum + dot(value_end_ref[:, lanes], read_high, 1, 1)
        read_sum = read_sum + dot(delta_start_ref[:, lanes], write_low, 1, 1)
        read_sum = read_sum + dot(delta_end_ref[:, lanes], write_high, 1, 1)
    work_ref[:, half : half + STATE] = write_sum
    work_ref[:, half + STATE :] = read_sum
    tokens = mine_ref.shape[0]
    mine_ref[...] = work_ref[pl.ds(pl.multiple_of(core_ref[0] * tokens, tokens), tokens), :]
    send_ref[...] = work_ref[
        pl.ds(pl.multiple_of((1 - core_ref[0]) * tokens, tokens), tokens), :
    ].astype(bf16)


def tail(core, back, write, value_start, value_end, delta_start, delta_end, fades, base):
    rows, width = base.shape
    vmem = pl.BlockSpec(memory_space=pltpu.VMEM)
    return pl.pallas_call(
        tail_kernel,
        in_specs=[pl.BlockSpec(memory_space=pltpu.SMEM)] + [vmem] * 9,
        out_shape=(
            jax.ShapeDtypeStruct((rows // 2, width), f32),
            jax.ShapeDtypeStruct((rows // 2, width), bf16),
        ),
        scratch_shapes=[pltpu.VMEM((rows, width), f32)],
    )(core.reshape(1), back, write, value_start, value_end, delta_start, delta_end, *fades, base)


def to_message(low, high):
    def cut(a):
        n, w = a.shape
        return a.astype(bf16).reshape(n // 8, 8, w // 128, 128).transpose(2, 0, 1, 3)

    both = jnp.stack([cut(low), cut(high)], axis=2)
    return both.reshape(-1, 16, 128)


def on_device(
    layer_input,
    cotangent,
    routes,
    route_weight,
    gate_weight,
    up_weight,
    down_weight,
    heads_value,
    output_gate,
    mixer_saved,
    proj_weight,
    state_write,
    state_read,
    decay_rate,
):
    core = lax.axis_index(CORE)
    tp = lax.axis_index(TP)
    first = core == 0
    tokens, width = layer_input.shape
    chips = lax.axis_size(CHIPS)
    experts = 2 * chips
    cap = max(2, 3 * tokens * routes.shape[1] // (2 * experts))
    rows = 2 * cap
    n_tp = lax.axis_size(TP)
    heads = decay_rate.shape[1]
    half_heads = heads // 2
    half = heads_value.shape[1] // 2

    def ordered(mine, other, axis=0):
        return jnp.concatenate(
            [jnp.where(first, mine, other), jnp.where(first, other, mine)], axis=axis
        )

    def halves(a):
        left, right = a[:, : a.shape[1] // 2], a[:, a.shape[1] // 2 :]
        return jnp.where(first, left, right), jnp.where(first, right, left)

    small = jnp.concatenate([routes.T.astype(f32), route_weight.T, decay_rate.T], axis=0)
    small_other = swap(small)
    input_other = swap(layer_input)
    cotangent_other = swap(cotangent)
    sent, spot = route(
        core,
        small,
        small_other,
        layer_input,
        input_other,
        cotangent,
        cotangent_other,
        chips,
        rows,
    )
    later_inputs = (gate_weight, up_weight, down_weight, heads_value, output_gate, mixer_saved)
    later_inputs += (proj_weight, state_write, state_read, small, small_other)
    sent, later_inputs = lax.optimization_barrier((sent, later_inputs))
    gate_weight, up_weight, down_weight, heads_value, output_gate, mixer_saved = later_inputs[:6]
    proj_weight, state_write, state_read, small, small_other = later_inputs[6:]

    spot_row = lax.broadcasted_iota(jnp.int32, (chips * 2 * rows, 2 * tokens), 0)
    back = [
        sum(
            jnp.where((spot[k : k + 1] >= 0) & (spot_row == spot[k : k + 1] + j * rows), 1.0, 0.0)
            for k in range(2)
        ).astype(bf16)
        for j in range(2)
    ]

    active_gate, slope_gate = silu_parts(output_gate.astype(f32))
    saved = mixer_saved.astype(f32)
    gated = (saved * active_gate).astype(bf16)
    value_mine, value_send = halves(heads_value)
    side = jnp.concatenate([value_send, state_write, state_read, gated], axis=1)
    side_other = swap(side)
    slots = chips * rows
    slots = chips * rows
    out_row = lax.broadcasted_iota(jnp.int32, (slots, 2 * slots), 0)
    in_row = lax.broadcasted_iota(jnp.int32, (slots, 2 * slots), 1)
    origin = out_row + out_row // rows * rows
    sort_rows = [(origin + j * rows == in_row).astype(bf16) for j in range(2)]
    side_other, small, small_other, back, sort_rows = lax.optimization_barrier(
        (side_other, small, small_other, back, sort_rows)
    )
    value = ordered(value_mine, side_other[:, :half])
    gated_all = jnp.concatenate([gated, side_other[:, half + 2 * STATE :]], axis=0)
    write = ordered(state_write, side_other[:, half : half + STATE])
    read = ordered(state_read, side_other[:, half + STATE : half + 2 * STATE])
    rates = ordered(
        *(jnp.where(first, a[4 : 4 + half_heads], a[4 + half_heads :]) for a in (small, small_other)),
        axis=1,
    )
    cumul_row = jnp.cumsum(rates, axis=1)
    head_of = lax.broadcasted_iota(jnp.int32, (half_heads, half), 0) * HEAD_DIM
    lane = lax.broadcasted_iota(jnp.int32, (half_heads, half), 1)
    spread_heads = ((lane >= head_of) & (lane < head_of + HEAD_DIM)).astype(f32)
    cumul_wide = lax.dot_general(
        cumul_row,
        spread_heads,
        (((0,), (0,)), ((), ())),
        precision=lax.Precision.HIGHEST,
        preferred_element_type=f32,
    )
    total_wide = cumul_wide[-1:]
    fade_end = jnp.exp(cumul_wide - total_wide)
    fade_start = jnp.exp(-cumul_wide)
    value_f = value.astype(f32)
    value_end = (value_f * fade_end).astype(bf16)
    value_start = (value_f * fade_start).astype(bf16)
    write_states = to_message(dot(write, value_end, 0, 0), dot(write, value_start, 0, 0))
    total_high = lax.reduce_precision(total_wide, 8, 7)
    row = lax.broadcasted_iota(jnp.int32, (8, half), 0)
    total_low = total_wide - total_high
    total_rows = jnp.where(row == 0, total_high, jnp.where(row == 1, total_low, 0.0)).astype(bf16)
    total_rows = total_rows.reshape(8, half // 128, 1, 128).transpose(1, 2, 0, 3)
    total_rows = jnp.broadcast_to(total_rows, (half // 128, STATE // 8, 8, 128))
    total_rows = total_rows.reshape(-1, 8, 128)
    quarter = width

    def rolled(a):
        parts = a.reshape(n_tp, quarter, a.shape[1])
        return [
            lax.dynamic_index_in_dim(parts, (tp + i) & (n_tp - 1), 0, keepdims=False)
            for i in range(n_tp)
        ]

    def unrolled(parts):
        stack = jnp.stack(parts)
        return [
            lax.dynamic_index_in_dim(stack, (k + n_tp - tp) & (n_tp - 1), 0, keepdims=False)
            for k in range(n_tp)
        ]

    gate_up = [
        jnp.concatenate(pair, axis=1) for pair in zip(rolled(gate_weight[0]), rolled(up_weight[0]))
    ]
    down = [
        lax.dynamic_slice_in_dim(down_weight[0], ((tp + i) & (n_tp - 1)) * quarter, quarter, 1)
        for i in range(n_tp)
    ]
    proj = rolled(proj_weight)
    hid = gate_weight.shape[2]
    received = exchange(sent.reshape(chips, 2 * rows, width)).reshape(2 * slots, width)
    ready = (write, read, value, gated_all, fade_end, fade_start, value_end, value_start)
    ready += (write_states, total_rows, cumul_wide, cumul_row)
    received, ready = lax.optimization_barrier((received, ready))
    write, read, value, gated_all, fade_end, fade_start, value_end, value_start = ready[:8]
    write_states, total_rows, cumul_wide, cumul_row = ready[8:]
    input_own, cotangent_own = (dot(a, received).astype(bf16) for a in sort_rows)
    input_low = ring(input_own, 1)
    cotangent_up = ring(cotangent_own, -1)
    input_up = ring(input_own, -1)
    cotangent_low = ring(cotangent_own, 1)
    input_far = ring(input_low, 1)
    cotangent_far = ring(cotangent_up, -1)
    input_parts = [input_own, input_up, input_far, input_low]
    cotangent_parts = [cotangent_own, cotangent_up, cotangent_far, cotangent_low]
    order = (0, 1, 3, 2)
    pre = sum(dot(input_parts[i], gate_up[i]) for i in order)
    hidden_grad = sum(dot(cotangent_parts[i], down[i], 1, 1) for i in order)
    pre_gate, pre_up = pre[:, :hid], pre[:, hid:]
    active, slope = silu_parts(pre_gate)
    hidden = (active * pre_up).astype(bf16)
    deltas = jnp.concatenate(
        [(hidden_grad * pre_up * slope).astype(bf16), (hidden_grad * active).astype(bf16)], axis=1
    )
    opposite = ring(dot(deltas, gate_up[2], 1, 1).astype(bf16), 2)
    right, left, own = (dot(deltas, gate_up[i], 1, 1).astype(bf16) for i in (1, 3, 0))
    returned = spread(own, ring(right, 1), ring(left, -1), opposite)
    returned, deltas, hidden = lax.optimization_barrier((returned, deltas, hidden))
    cut = width // 2
    arrived = exchange(returned.reshape(chips, 2 * rows, cut))
    arrived = arrived.reshape(2 * slots, cut)

    both_grad = unrolled([dot(input_parts[i], deltas, 0, 0).astype(bf16) for i in range(n_tp)])
    gate_grad = jnp.concatenate([a[:, :hid] for a in both_grad], axis=0)[None]
    up_grad = jnp.concatenate([a[:, hid:] for a in both_grad], axis=0)[None]
    down_grad = jnp.concatenate(
        unrolled([dot(hidden, cotangent_parts[i], 0, 0).astype(bf16) for i in range(n_tp)]), axis=1
    )[None]

    arrived, gate_grad, up_grad, down_grad = lax.optimization_barrier(
        (arrived, gate_grad, up_grad, down_grad)
    )
    summed = jnp.concatenate([dot(back[0], arrived, 0, 0), dot(back[1], arrived, 0, 0)], axis=1)
    summed_other = swap(summed[tokens:].astype(bf16)).astype(f32)
    layer_grad = (cotangent.astype(f32) + summed[:tokens] + summed_other).astype(bf16)
    grads = [layer_grad, ring(layer_grad, -1), ring(layer_grad, 2), ring(layer_grad, 1)]
    out_delta = sum(dot(grads[i], proj[i]) for i in (0, 1, 3, 2)).astype(bf16).astype(f32)
    outgate_grad = (out_delta * saved * slope_gate).astype(bf16)
    mixer_delta = (out_delta * active_gate).astype(bf16)
    delta_mine, delta_send = halves(mixer_delta)
    delta = ordered(delta_mine, swap(delta_send))
    delta_f = delta.astype(f32)
    delta_end = (delta_f * fade_end).astype(bf16)
    delta_start = (delta_f * fade_start).astype(bf16)
    read_states = to_message(dot(read, delta_end, 0, 0), dot(read, delta_start, 0, 0))
    states_got = exchange(jnp.concatenate([read_states, write_states, total_rows], axis=1))

    grad_mine = jnp.concatenate(grads, axis=1)
    grad_all = jnp.concatenate([grad_mine, swap(grad_mine)], axis=0)
    proj_part = dot(grad_all, gated_all, 0, 0).astype(bf16)
    deep, wide = lax.axis_size(SP[0]), lax.axis_size(SP[1])
    block = proj_part.shape[0] // chips // 2
    across = lax.axis_index(SP[1])
    pieces = proj_part.reshape(n_tp, deep // n_tp, wide, 2, block, width)
    pieces = lax.dynamic_index_in_dim(pieces, core, 3, keepdims=False)
    proj_part = jnp.stack(unrolled([pieces[i] for i in range(n_tp)]))
    proj_sum = ring_reduce(
        [
            lax.dynamic_index_in_dim(
                proj_part, (across + i) & (wide - 1), 2, keepdims=False
            ).reshape(deep, block, width)
            for i in range(wide)
        ],
        SP[1],
    )
    scanned = scan_chunks(states_got)
    states_back = exchange(scanned)
    depth = lax.axis_index(SP[0])
    level = depth >> 1
    count = deep // 2
    levels = proj_sum.reshape(count, 2, block, width)

    def level_part(i):
        return lax.dynamic_index_in_dim(levels, (level + i) & (count - 1), 0, keepdims=False)

    others = [
        lax.ppermute(
            level_part(k).astype(bf16), SP[0], [(i, (i + 2 * k) % deep) for i in range(deep)]
        )
        for k in range(1, count)
    ]
    upper = (depth & 1) != 0
    pair = level_part(0) + sum(a.astype(f32) for a in others)
    away = jnp.where(upper, pair[0], pair[1]).astype(bf16)
    got = lax.ppermute(away, SP[0], [(i, i ^ 1) for i in range(deep)])
    proj_grad = jnp.where(upper, pair[1], pair[0]) + got.astype(f32)

    base = mix_chunk(delta, value, write, read, cumul_wide, cumul_row)
    outs_mine, outs_send = tail(
        core,
        states_back,
        write,
        value_start,
        value_end,
        delta_start,
        delta_end,
        (fade_start, fade_end),
        base,
    )
    outs_got = swap(outs_send)
    value_out, write_out, read_out = join(core, outs_mine, outs_got)
    return (
        gate_grad,
        up_grad,
        down_grad,
        proj_grad,
        value_out,
        write_out,
        read_out,
        outgate_grad,
    )


def solution(mesh):
    split = Mesh(mesh.devices.reshape(8, 4, 2, mesh.shape["tp"]), SP + (TP,))
    placed = (
        P(SP, TP),
        P(SP, TP),
        P(SP, None),
        P(SP, None),
        P(SP, None, TP),
        P(SP, None, TP),
        P(SP, TP, None),
        P(SP, TP),
        P(SP, TP),
        P(SP, TP),
        P(None, TP),
        P(SP, TP),
        P(SP, TP),
        P(SP, TP),
    )

    return jax.shard_map(
        on_device,
        mesh=split,
        in_specs=placed,
        out_specs=(
            P(SP, None, TP),
            P(SP, None, TP),
            P(SP, TP, None),
            P(SP, TP),
            P(SP, TP),
            P(SP, TP),
            P(SP, TP),
            P(SP, TP),
        ),
        check_vma=False,
    )
```
